32 devices in a mesh: ep: 8 (over z, y), tp: 4 (over x, core).
Axes of the slice: x: 2, y: 2, z: 4, core: 2. Of those that a mesh axis runs over, the one named last changes fastest.
Arguments:
- tokens: bfloat16 [2560, 2048], P('ep'), may hold values from -12 to 12, as said below
- cotangent: bfloat16 [2560, 2048], P('ep'), may hold values from -0.59765625 to 0.59765625
- route_ids: int32 [2560, 2], P('ep'), may hold values from 0 to 7, all different within a row; in each aligned block of 320 rows (0 to 319, 320 to 639, ...) at most 160 rows name the same one
- route_weights: bfloat16 [2560, 2], P('ep'), may hold values from 0.049804688 to 1
- w_gate: bfloat16 [8, 2048, 2048], P('ep', None, 'tp'), may hold values from -0.125 to 0.125
- w_up: bfloat16 [8, 2048, 2048], P('ep', None, 'tp'), may hold values from -0.125 to 0.125
- w_down: bfloat16 [8, 2048, 2048], P('ep', 'tp'), may hold values from -0.125 to 0.125
- dense_in: bfloat16 [2048, 256], P(('ep', 'tp')), may hold values from -0.125 to 0.125
- dense_out: bfloat16 [2048, 256], P(('ep', 'tp')), may hold values from -0.375 to 0.375
- dense_gate: bfloat16 [2048], replicated, may hold values from -0.125 to 0.125
Outputs:
- grad_tokens: bfloat16 [2560, 2048], P('ep', 'tp')
- grad_route_weights: bfloat16 [2560, 2], P('ep')
- grad_gate: float32 [8, 2048, 2048], P('ep', None, 'tp')
- grad_up: float32 [8, 2048, 2048], P('ep', None, 'tp')
- grad_down: float32 [8, 2048, 2048], P('ep', 'tp')
- grad_dense_in: float32 [2048, 256], P(('ep', 'tp'))
- grad_dense_out: float32 [2048, 256], P(('ep', 'tp'))
- grad_dense_gate: float32 [2048], P(('ep', 'tp'))
The draws below stay inside these ranges and needn't reach their ends.
Inputs may be any that keep to these rules, and one draw needn't show every extreme that they name: `route_ids`: each row names 2 different experts; among the rows of one index of ep no expert is named more than 160 times, and that count is reached. `tokens`: rows carry scales between 0.5 and 2 that differ from row to row.
All inputs are finite; a program needn't handle non-finite values.
Results may differ from the reference program's by a relative error of at most 0.01.
Values may be sent and summed in bfloat16 or wider, within the bound.
A program may use at most 128 MiB of HBM per device.

```python
import math
import jax
import jax.numpy as jnp
import numpy as np
from jax import lax

D = 2048
FF = 2048
R = 256
TOP = 2
TOK_DEV = 320
EXPERTS = 8
CAP = 160
TOKENS = 2560
N_EP = 8
N_TP = 4


def draw_tokens(key, part):
    base_key = jax.random.fold_in(key, 11)
    scale_key = jax.random.fold_in(key, 12)
    scales = jnp.exp(jax.random.uniform(scale_key, (TOKENS, 1), jnp.float32, math.log(0.5), math.log(2.0)))
    base = jax.random.normal(base_key, (TOKENS, D), jnp.float32)
    base = jnp.clip(base, -6.0, 6.0)
    return (base * scales).astype(jnp.bfloat16)


def levels(own_key, extent, pieces, low, top_value):
    def one(dim, blocks):
        draws = jax.random.uniform(jax.random.fold_in(jax.random.fold_in(own_key, 6), dim), (blocks,), jnp.float32, low / len(pieces), top_value / len(pieces))
        return jnp.repeat(jnp.exp(draws), extent[dim] // blocks).reshape((-1,) + (1,) * (len(extent) - dim - 1))

    loudness = one(*pieces[0])
    for cut in pieces[1:]:
        loudness = loudness * one(*cut)
    return loudness


def routed_block(rng, own, number, rows, number_of, top, limit, slope):
    order = jax.random.permutation(rng, number_of)
    crowded, common = shares(number_of, rows * top, limit, slope, True), shares(number_of, rows * top, limit, slope, False)
    places = jnp.arange(number_of)

    def named(lengths, offset_by):
        used = int((lengths > 0).sum())
        fixed = max(1, used // 4)
        passed = fixed + (places - fixed + offset_by * (used - fixed)) % max(1, number_of - fixed)
        return jnp.zeros((number_of,), jnp.int32).at[order[jnp.where(places < fixed, places, passed)]].set(jnp.asarray(lengths, jnp.int32))

    lengths = jnp.where(number % 4 == 0, named(crowded, number // 4), named(common, number - number // 4 - 1))
    mixed = jax.random.permutation(jax.random.fold_in(own, 3), number_of)
    giver, receiver = mixed[0:number_of // 2 * 2:2], mixed[1:number_of // 2 * 2:2]
    margin = jnp.minimum(lengths[giver] - 1, limit - lengths[receiver]) // 2
    margin = jnp.where((giver == order[0]) | (receiver == order[0]) | (lengths[receiver] == 0), 0, jnp.maximum(margin, 0))
    passed = jax.random.randint(jax.random.fold_in(own, 4), (number_of // 2,), 0, 1 << 20) % (margin + 1)
    lengths = lengths.at[giver].add(-passed).at[receiver].add(passed)
    items = jnp.searchsorted(jnp.cumsum(lengths), jnp.arange(rows * top), side="right").astype(jnp.int32)
    grid = items.reshape(top, rows).T
    grid = grid[jax.random.permutation(jax.random.fold_in(own, 1), rows)]
    offset_by = jax.random.randint(jax.random.fold_in(own, 2), (rows, 1), 0, top)
    return jnp.take_along_axis(grid, (jnp.arange(top)[None, :] + offset_by) % top, axis=1)


def shares(amount, total, limit, skew, full):
    weights = [(1 << 20) // math.isqrt(rank ** skew) + 1 for rank in range(1, amount + 1)]
    largest = limit if full else min(limit, max(-(-total // amount), total * weights[0] // sum(weights)))
    least = 1 if total - largest >= amount - 1 else 0
    given, rest = [largest] + [least] * (amount - 1), total - largest - least * (amount - 1)
    while rest > 0:
        free = [i for i in range(1, amount) if given[i] < largest] or [i for i in range(1, amount) if given[i] < limit]
        whole, left = sum([weights[i] for i in free]), rest
        for i in free:
            extra = min(limit - given[i], max(1, left * weights[i] // whole), rest)
            given[i] = given[i] + extra
            rest = rest - extra
    return np.array(given)


def scatter_about(stream_key, shape, deviation, most, split=(), kind=jnp.bfloat16):
    values = jax.random.normal(stream_key, shape, jnp.float32) * deviation
    if len(split) > 0:
        values = levels(stream_key, shape, split, -0.22, 0.18) * values
    return jnp.clip(values, min=-most, max=most).astype(kind)


def setup_inputs(seed: int = 0) -> dict:
    keys = jax.random.split(jax.random.key(seed), 11)
    tokens = draw_tokens(jax.random.fold_in(keys[10], 71), 0)
    cotangent = scatter_about(keys[1], (TOKENS, D), 0.1, 0.59765625, ((0, 8),))
    route_ids_keys = jax.random.split(jax.random.fold_in(keys[2], 1), TOKENS // TOK_DEV)
    route_ids_turns = jax.random.permutation(jax.random.fold_in(keys[2], 3), TOKENS // TOK_DEV)
    route_ids = jax.vmap(lambda own, number: routed_block(jax.random.fold_in(keys[2], 2), own, number, TOK_DEV, EXPERTS, TOP, CAP, 2))(route_ids_keys, route_ids_turns).reshape((TOKENS, TOP))
    route_weights = jnp.clip(0.049804688 + 0.9501953 * jax.random.uniform(keys[3], (TOKENS, TOP), jnp.float32) ** levels(keys[3], (TOKENS, TOP), ((0, 8),), -0.2, 0.2), 0.049804688, 1.0).astype(jnp.bfloat16)
    w_gate = scatter_about(keys[4], (EXPERTS, D, FF), D ** -0.5, 0.125, ((0, 8), (2, 4)))
    w_up = scatter_about(keys[5], (EXPERTS, D, FF), D ** -0.5, 0.125, ((0, 8), (2, 4)))
    w_down = scatter_about(keys[6], (EXPERTS, FF, D), FF ** -0.5, 0.125, ((0, 8), (1, 4)))
    dense_in = scatter_about(keys[7], (D, R), D ** -0.5, 0.125, ((0, 32),))
    dense_out = scatter_about(keys[8], (D, R), R ** -0.5, 0.375, ((0, 32),))
    dense_gate = scatter_about(keys[9], (D,), D ** -0.5, 0.125)
    return dict(tokens=tokens, cotangent=cotangent, route_ids=route_ids, route_weights=route_weights, w_gate=w_gate, w_up=w_up, w_down=w_down, dense_in=dense_in, dense_out=dense_out, dense_gate=dense_gate)


CLAMP_LIMIT = 7.0
SIG_SLOPE = 1.702


def expert_grads(packed):
    x_rows, dy_rows, weight_rows, gate_w, up_w, down_w = packed
    gate_pre = jnp.dot(x_rows, gate_w, preferred_element_type=jnp.float32)
    up_pre = jnp.dot(x_rows, up_w, preferred_element_type=jnp.float32)
    gate_clamp = jnp.minimum(gate_pre, CLAMP_LIMIT)
    up_clamp = jnp.clip(up_pre, -CLAMP_LIMIT, CLAMP_LIMIT)
    sig = jax.nn.sigmoid(SIG_SLOPE * gate_clamp)
    act = (gate_clamp * sig * (up_clamp + 1.0)).astype(jnp.bfloat16)
    back = lax.dot_general(dy_rows, down_w, (((1,), (1,)), ((), ())), preferred_element_type=jnp.float32)
    weight_grad = jnp.sum(act.astype(jnp.float32) * back, axis=1).astype(jnp.bfloat16)
    route_col = weight_rows.astype(jnp.float32)[:, None]
    d_act = route_col * back
    d_gate = jnp.where(gate_pre < CLAMP_LIMIT, d_act * (up_clamp + 1.0) * (sig + SIG_SLOPE * gate_clamp * sig * (1.0 - sig)), 0.0).astype(jnp.bfloat16)
    d_up = jnp.where(jnp.abs(up_pre) < CLAMP_LIMIT, d_act * gate_clamp * sig, 0.0).astype(jnp.bfloat16)
    scaled_cot = (route_col * dy_rows.astype(jnp.float32)).astype(jnp.bfloat16)
    contract_rows = (((0,), (0,)), ((), ()))
    grad_gate = lax.dot_general(x_rows, d_gate, contract_rows, preferred_element_type=jnp.float32)
    grad_up = lax.dot_general(x_rows, d_up, contract_rows, preferred_element_type=jnp.float32)
    grad_down = lax.dot_general(act, scaled_cot, contract_rows, preferred_element_type=jnp.float32)
    slot_count, hidden = d_gate.shape
    model_width = gate_w.shape[0]
    group = hidden // N_TP
    partials = jnp.einsum('sjf,djf->jsd', d_gate.astype(jnp.float32).reshape(slot_count, N_TP, group), gate_w.astype(jnp.float32).reshape(model_width, N_TP, group))
    partials = partials + jnp.einsum('sjf,djf->jsd', d_up.astype(jnp.float32).reshape(slot_count, N_TP, group), up_w.astype(jnp.float32).reshape(model_width, N_TP, group))
    rounded = lax.optimization_barrier(partials.astype(jnp.bfloat16))
    row_grad = jnp.sum(rounded.astype(jnp.float32), axis=0).astype(jnp.bfloat16)
    return grad_gate, grad_up, grad_down, row_grad, weight_grad


def reference(tokens, cotangent, route_ids, route_weights, w_gate, w_up, w_down, dense_in, dense_out, dense_gate):
    total_tokens, model_width = tokens.shape
    top_k = route_ids.shape[1]
    expert_count = w_gate.shape[0]
    per_device = total_tokens // N_EP
    ids = route_ids.reshape(N_EP, per_device * top_k).astype(jnp.int32)
    one_hot = (ids[:, :, None] == jnp.arange(expert_count, dtype=jnp.int32)[None, None, :]).astype(jnp.int32)
    earlier = jnp.cumsum(one_hot, axis=1) - one_hot
    slot_index = jnp.sum(earlier * one_hot, axis=2)
    source_dev = jnp.arange(N_EP, dtype=jnp.int32)[:, None]
    position = (ids * (N_EP * CAP) + source_dev * CAP + slot_index).reshape(-1).astype(jnp.int32)
    token_of = (jnp.arange(total_tokens * top_k, dtype=jnp.int32) // top_k).astype(jnp.int32)
    slot_total = expert_count * N_EP * CAP
    x_buf = jnp.zeros((slot_total, model_width), jnp.bfloat16).at[position].set(tokens[token_of]).reshape(expert_count, N_EP * CAP, model_width)
    dy_buf = jnp.zeros((slot_total, model_width), jnp.bfloat16).at[position].set(cotangent[token_of]).reshape(expert_count, N_EP * CAP, model_width)
    weight_buf = jnp.zeros((slot_total,), jnp.bfloat16).at[position].set(route_weights.reshape(-1)).reshape(expert_count, N_EP * CAP)
    grad_gate, grad_up, grad_down, row_grad, weight_grad = lax.map(expert_grads, (x_buf, dy_buf, weight_buf, w_gate, w_up, w_down))
    expert_dx = row_grad.reshape(slot_total, model_width)[position].astype(jnp.float32).reshape(total_tokens, top_k, model_width)
    expert_dx = jnp.sum(expert_dx, axis=1)
    grad_route_weights = weight_grad.reshape(-1)[position].reshape(total_tokens, top_k)

    dense_pre = jnp.dot(tokens, dense_in, preferred_element_type=jnp.float32)
    dense_act = jax.nn.silu(dense_pre).astype(jnp.bfloat16)
    dense_val = lax.dot_general(dense_act, dense_out, (((1,), (1,)), ((), ())), preferred_element_type=jnp.float32)
    mix = jax.nn.sigmoid(jnp.dot(tokens, dense_gate, preferred_element_type=jnp.float32))
    cot_wide = cotangent.astype(jnp.float32)
    dense_scaled = (mix[:, None] * cot_wide).astype(jnp.bfloat16)
    dense_back = jnp.dot(dense_scaled, dense_out, preferred_element_type=jnp.float32)
    sig_pre = jax.nn.sigmoid(dense_pre)
    dense_dpre = (dense_back * sig_pre * (1.0 + dense_pre * (1.0 - sig_pre))).astype(jnp.bfloat16)
    dlogit = mix * (1.0 - mix) * jnp.sum(cot_wide * dense_val, axis=1)
    dense_dx = lax.dot_general(dense_dpre, dense_in, (((1,), (1,)), ((), ())), preferred_element_type=jnp.float32)
    dense_dx = dense_dx + dlogit[:, None] * dense_gate.astype(jnp.float32)[None, :]
    grad_tokens = (dense_dx + expert_dx).astype(jnp.bfloat16)
    contract_rows = (((0,), (0,)), ((), ()))
    grad_dense_in = lax.dot_general(tokens, dense_dpre, contract_rows, preferred_element_type=jnp.float32)
    grad_dense_out = lax.dot_general(dense_scaled, dense_act, contract_rows, preferred_element_type=jnp.float32)
    grad_dense_gate = jnp.sum(tokens.astype(jnp.float32) * dlogit[:, None], axis=0)
    return (grad_tokens, grad_route_weights, grad_gate, grad_up, grad_down, grad_dense_in, grad_dense_out, grad_dense_gate)
```

```python
import functools
import types

import jax
import jax.numpy as jnp
from jax import lax
from jax.experimental import pallas as pl
from jax.experimental.pallas import tpu as pltpu
from jax.sharding import PartitionSpec as P

CLAMP_LIMIT = 7.0
SIG_SLOPE = 1.702
MESH = pl.DeviceIdType.MESH
ANY = pl.BlockSpec(memory_space=pl.ANY)
VMEM = pl.BlockSpec(memory_space=pltpu.VMEM)
CONTRACT_COLS = (((1,), (1,)), ((), ()))
CONTRACT_ROWS = (((0,), (0,)), ((), ()))
F32 = jnp.float32
BF = jnp.bfloat16


def layer_kernel(n_ep, n_tp, names, *refs):
    r = types.SimpleNamespace(**dict(zip(names, refs)))
    me = lax.axis_index("ep")
    t = lax.axis_index("tp")
    half = t // 2
    side = t % 2
    t_core = half * 2 + 1 - side
    t_x = (1 - half) * 2 + side
    cap, cols = r.x_send.shape[1:]
    tok_dev, width = r.tok.shape
    top_k = r.ids.shape[0]
    lanes = r.w_all.shape[2]
    core_peer = (me, t_core)
    x_peer = (me, t_x)
    log = n_ep.bit_length() - 1

    def dst(k):
        if 1 << log != n_ep:
            return lax.rem(me + k, n_ep)
        out = me
        for b in range(log):
            bit = (k // (1 << b)) % 2
            out = out + bit * (1 << b) * (1 - 2 * ((me // (1 << b)) % 2))
        return out

    def src(k):
        if 1 << log != n_ep:
            return lax.rem(me + n_ep - k, n_ep)
        return dst(k)

    def quarter(q):
        return pl.ds(pl.multiple_of(q * cols, cols), cols)

    def remote(source, target, sems, device):
        return pltpu.make_async_remote_copy(
            src_ref=source,
            dst_ref=target,
            send_sem=sems[0],
            recv_sem=sems[1],
            device_id=device,
            device_id_type=MESH,
        )

    loads = [
        pltpu.make_async_copy(a, b, r.load_sem.at[n])
        for n, (a, b) in enumerate(
            (
                (r.in_own, r.dense_all.at[me, t, 0]),
                (r.out_own, r.dense_all.at[me, t, 1]),
                (r.tokens, r.tok),
                (r.cotangent, r.cot),
                (r.w_gate, r.gate_w),
                (r.w_up, r.up_w),
                (r.w_down, r.down_w),
            )
        )
    ]
    for c in loads:
        c.start()

    peers = [(dst(k), t) for k in range(1, n_ep)] + [core_peer, x_peer]
    barrier = pltpu.get_barrier_semaphore()
    for device in peers:
        pl.semaphore_signal(barrier, inc=1, device_id=device, device_id_type=MESH)

    experts = r.pos.shape[0]
    expert_row = lax.broadcasted_iota(jnp.int32, (experts, tok_dev), 0)
    member = jnp.zeros((experts, tok_dev), F32)
    weight = jnp.zeros((experts, tok_dev), F32)
    for k in range(top_k):
        hit = r.ids[k : k + 1, :] == expert_row
        member = jnp.where(hit, 1.0, member)
        weight = jnp.where(hit, r.route[k : k + 1, :].astype(F32), weight)
    below = lax.broadcasted_iota(jnp.int32, (tok_dev, tok_dev), 0) < lax.broadcasted_iota(
        jnp.int32, (tok_dev, tok_dev), 1
    )
    rank = jnp.dot(
        member.astype(BF), jnp.where(below, 1.0, 0.0).astype(BF), preferred_element_type=F32
    )
    r.pos[...] = jnp.where(member > 0.0, rank, -1.0)
    r.weight[...] = weight
    r.w_send[...] = jnp.zeros(r.w_send.shape, F32)

    pl.semaphore_wait(barrier, len(peers))

    rows_send = (r.x_send, r.dy_send)
    rows_all = (r.x_all, r.dy_all)

    def shard_hop(kind, k):
        i = src(k)
        sems = (r.send_shard.at[kind, k], r.recv_shard.at[kind, k])
        if kind == 0:
            block = r.dense_all.at[me, t]
            return remote(block, block, sems, (dst(k), t))
        block = r.dense_all.at[i, t_x if kind == 3 else t]
        return remote(block, block, sems, x_peer if kind == 1 else core_peer)

    def row_hop(a, kind, k):
        i = src(k)
        sems = (r.send_rows.at[a, kind, k], r.recv_rows.at[a, kind, k])
        if kind == 0:
            return remote(
                rows_send[a].at[k], rows_all[a].at[me, :, quarter(t)], sems, (dst(k), t)
            )
        block = rows_all[a].at[i, :, quarter(t_x if kind == 3 else t)]
        return remote(block, block, sems, x_peer if kind == 1 else core_peer)

    def w_hop(k):
        return remote(
            r.w_send.at[k], r.w_all.at[me], (r.send_w.at[k], r.recv_w.at[k]), (dst(k), t)
        )

    loads[0].wait()
    loads[1].wait()
    shard_hop(1, 0).start()
    shard_hop(2, 0).start()

    @pl.loop(1, n_ep)
    def _(k):
        shard_hop(0, k).start()

    loads[2].wait()
    loads[3].wait()
    slot = lax.broadcasted_iota(jnp.int32, (cap, tok_dev), 0).astype(F32)

    def pick_rows(e):
        pick = jnp.where(slot == r.pos[pl.ds(e, 1), :], 1.0, 0.0).astype(BF)
        r.picks[e] = pick
        wide = jnp.broadcast_to(r.weight[pl.ds(e, 1), :], (16, tok_dev)).astype(BF)
        sent = lax.dot_general(wide, pick, CONTRACT_COLS, preferred_element_type=F32)
        return pick, sent[:8]

    @pl.loop(1, n_ep + 1)
    def _(k):
        @pl.when(k < n_ep)
        def _():
            pick, sent = pick_rows(dst(k))
            r.w_send[k, :, :cap] = sent
            r.x_send[k] = jnp.dot(
                pick, r.tok[:, quarter(t)], preferred_element_type=F32
            ).astype(BF)
            r.dy_send[k] = jnp.dot(
                pick, r.cot[:, quarter(t)], preferred_element_type=F32
            ).astype(BF)

        @pl.when(k > 1)
        def _():
            w_hop(k - 1).start()
            for a in range(2):
                row_hop(a, 0, k - 1).start()

    pick, sent = pick_rows(me)
    r.w_all[me] = jnp.zeros((8, lanes), F32)
    r.w_all[me, :, :cap] = sent

    @pl.loop(0, n_tp)
    def _(q):
        r.x_all[me, :, quarter(q)] = jnp.dot(
            pick, r.tok[:, quarter(q)], preferred_element_type=F32
        ).astype(BF)
        r.dy_all[me, :, quarter(q)] = jnp.dot(
            pick, r.cot[:, quarter(q)], preferred_element_type=F32
        ).astype(BF)

    for c in loads[4:]:
        c.wait()

    diagonal = lax.broadcasted_iota(jnp.int32, (cap, lanes), 0) == lax.broadcasted_iota(
        jnp.int32, (cap, lanes), 1
    )

    def compute(i):
        weight_row = r.w_all[i, 0:1]
        route_col = jnp.sum(jnp.where(diagonal, weight_row, 0.0), axis=1, keepdims=True)
        x_rows = r.x_all[i]
        gate_pre = jnp.dot(x_rows, r.gate_w[...], preferred_element_type=F32)
        up_pre = jnp.dot(x_rows, r.up_w[...], preferred_element_type=F32)
        gate_clamp = jnp.minimum(gate_pre, CLAMP_LIMIT)
        up_clamp = jnp.clip(up_pre, -CLAMP_LIMIT, CLAMP_LIMIT)
        sig = jax.nn.sigmoid(SIG_SLOPE * gate_clamp)
        act = (gate_clamp * sig * (up_clamp + 1.0)).astype(BF)
        r.act[i] = act
        dy_rows = r.dy_all[i]
        r.scaled[i] = (route_col * dy_rows.astype(F32)).astype(BF)
        back = lax.dot_general(dy_rows, r.down_w[...], CONTRACT_COLS, preferred_element_type=F32)
        weight_sum = jnp.sum(act.astype(F32) * back, axis=1, keepdims=True)
        r.w_part[pl.ds(i, 1), :] = jnp.sum(
            jnp.where(diagonal, weight_sum, 0.0), axis=0, keepdims=True
        )
        d_act = route_col * back
        d_gate = jnp.where(
            gate_pre < CLAMP_LIMIT,
            d_act * (up_clamp + 1.0) * (sig + SIG_SLOPE * gate_clamp * sig * (1.0 - sig)),
            0.0,
        ).astype(BF)
        d_up = jnp.where(jnp.abs(up_pre) < CLAMP_LIMIT, d_act * gate_clamp * sig, 0.0).astype(BF)
        r.d_gate[i] = d_gate
        r.d_up[i] = d_up
        part = lax.dot_general(d_gate, r.gate_w[...], CONTRACT_COLS, preferred_element_type=F32)
        part = part + lax.dot_general(
            d_up, r.up_w[...], CONTRACT_COLS, preferred_element_type=F32
        )
        r.part[i] = part.astype(BF)

    def back_core(k, h):
        return remote(
            r.part.at[src(k), :, quarter(h * 2 + 1 - side)],
            r.from_core.at[k, h],
            (r.send_bc.at[k, h], r.recv_bc.at[k, h]),
            core_peer,
        )

    def back_x(k):
        return remote(r.to_x.at[k], r.from_x.at[k], (r.send_bx.at[k], r.recv_bx.at[k]), x_peer)

    def back_ep(k):
        return remote(
            r.to_ep.at[k],
            r.rows_back.at[me],
            (r.send_be.at[k], r.recv_be.at[k]),
            (src(k), t),
        )

    def run(k):
        compute(src(k))
        for h in range(2):
            back_core(k, h).start()

    def sum_core(k):
        for h in range(2):
            back_core(k, h).wait_recv()
        other = r.part[src(k), :, quarter(t_x)].astype(F32)
        r.to_x[k] = (other + r.from_core[k, 1 - half].astype(F32)).astype(BF)
        back_x(k).start()

    def sum_x(k):
        back_x(k).wait_recv()
        mine = r.part[src(k), :, quarter(t)].astype(F32)
        mine = mine + r.from_core[k, half].astype(F32)
        return (mine + r.from_x[k].astype(F32)).astype(BF)

    def send_back(k):
        r.to_ep[k] = sum_x(k)
        back_ep(k).start()

    def grad_hop(k):
        return remote(
            r.dg_send.at[dst(k)], r.dg_back.at[me], (r.send_dg.at[k], r.recv_dg.at[k]), (dst(k), t)
        )

    def gate_hop(k):
        return remote(
            r.gg_send.at[dst(k)], r.gg_back.at[me], (r.send_gg.at[k], r.recv_gg.at[k]), (dst(k), t)
        )

    own_rows, rank_r = r.in_own.shape
    span = n_ep // n_tp
    block_cols = width // n_ep

    def dense():
        in_whole = r.dense_all[:, :, 0].reshape(width, rank_r)
        out_whole = r.dense_all[:, :, 1].reshape(width, rank_r)
        pre = jnp.dot(r.tok[...], in_whole, preferred_element_type=F32)
        cob = jnp.dot(r.cot[...], out_whole, preferred_element_type=F32)
        gate_wide = jnp.broadcast_to(r.gate_row[...].astype(F32), (16, width)).astype(BF)
        logit = lax.dot_general(
            r.tok[...], gate_wide, CONTRACT_COLS, preferred_element_type=F32
        )[:, :1]
        mix = jax.nn.sigmoid(logit)
        sig = jax.nn.sigmoid(pre)
        act = (pre * sig).astype(BF)
        dpre = (mix * cob * sig * (1.0 + pre * (1.0 - sig))).astype(BF)
        act_wide = act.astype(F32)
        dlogit = mix * (1.0 - mix) * jnp.sum(act_wide * cob, axis=1, keepdims=True)
        in_rows = r.dense_all[pl.ds(t * span, span), :, 0].reshape(cols, rank_r)
        dx = lax.dot_general(dpre, in_rows, CONTRACT_COLS, preferred_element_type=F32)
        r.dense_dx[...] = dx + dlogit * r.gate_row[:, quarter(t)].astype(F32)
        lane = lax.broadcasted_iota(jnp.int32, (tok_dev, 128), 1)
        high = dlogit.astype(BF).astype(F32)
        low = dlogit - high
        pair = jnp.where(lane == 0, high, jnp.where(lane == 1, low, 0.0)).astype(BF)
        gate_sum = lax.dot_general(pair, r.tok[...], CONTRACT_ROWS, preferred_element_type=F32)
        gate_sum = gate_sum[0:1] + gate_sum[1:2]
        for e in range(n_ep):
            r.gg_send[e, :, :block_cols] = jnp.broadcast_to(
                gate_sum[:, e * block_cols : (e + 1) * block_cols], (8, block_cols)
            )
        mixed = (mix * act_wide).astype(BF)
        for a, (left, right) in enumerate(((r.tok, dpre), (r.cot, mixed))):
            r.dense_grad[...] = lax.dot_general(
                left[...], right, CONTRACT_ROWS, preferred_element_type=F32
            )
            for e in range(n_ep):
                start = pl.multiple_of((e * n_tp + t) * own_rows, own_rows)
                r.dg_send[e, a] = r.dense_grad[pl.ds(start, own_rows), :].astype(BF)
        r.dg_back[me] = r.dg_send[me]
        r.gg_back[me] = r.gg_send[me]

        @pl.loop(1, n_ep)
        def _(k):
            gate_hop(k).start()
            grad_hop(k).start()

    shard_steps = (n_ep - 1 + 1) // 2

    @pl.loop(0, n_ep + 2)
    def _(n):
        for b in (2 * n - 1, 2 * n):

            @pl.when((b >= 1) & (b < n_ep))
            def _():
                shard_hop(0, b).wait_recv()
                shard_hop(1, b).start()
                shard_hop(2, b).start()

        @pl.when((n >= 1) & (n < n_ep))
        def _():
            for a in range(2):
                row_hop(a, 0, n).wait_recv()
                row_hop(a, 1, n).start()
                row_hop(a, 2, n).start()
            w_hop(n).wait_recv()

        @pl.when(n >= 3)
        def _():
            sum_core(n - 3)

        @pl.when(n == 4)
        def _():
            r.rows_back[me] = sum_x(0)

        @pl.when(n >= 5)
        def _():
            send_back(n - 4)

        @pl.when((n == 0) | (n >= 3))
        def _():
            k = jnp.where(n == 0, 0, n - 2)

            @pl.when(n >= 3)
            def _():
                for a in range(2):
                    for kind in (2, 3):
                        row_hop(a, kind, k).wait_recv()

            run(k)

        for b in (2 * n - 3, 2 * n - 2):

            @pl.when((b >= 0) & (b < n_ep))
            def _():
                shard_hop(1, b).wait_recv()
                shard_hop(3, b).start()

        @pl.when((n >= 2) & (n < n_ep + 1))
        def _():
            for a in range(2):
                row_hop(a, 1, n - 1).wait_recv()
                row_hop(a, 3, n - 1).start()

        @pl.when(n == shard_steps + 2)
        def _():
            @pl.loop(0, n_ep)
            def _(k):
                for kind in (2, 3):
                    shard_hop(kind, k).wait_recv()

            dense()

    rows = n_ep * cap
    stages = r.stage.shape[0]
    tiles = width // cols

    def tile_out(kind, j, slot_index):
        number = kind * tiles + j
        target = (
            r.grad_down.at[:, quarter(j)]
            if kind == 0
            else (r.grad_gate if kind == 1 else r.grad_up).at[quarter(j), :]
        )
        return pltpu.make_async_copy(
            r.stage.at[slot_index, : target.shape[0], : target.shape[1]],
            target,
            r.tile_sem.at[number],
        )

    def tile(kind, j):
        number = kind * tiles + j
        s = number % stages
        if number >= stages:
            old = number - stages
            tile_out(old // tiles, old % tiles, s).wait()
        if kind == 0:
            left = r.act[...].reshape(rows, -1)
            right = r.scaled.reshape(rows, width)[:, quarter(j)]
        else:
            left = r.x_all.reshape(rows, width)[:, quarter(j)]
            right = (r.d_gate if kind == 1 else r.d_up)[...].reshape(rows, -1)
        r.stage[s] = lax.dot_general(left, right, CONTRACT_ROWS, preferred_element_type=F32)
        tile_out(kind, j, s).start()

    def weight_core():
        return remote(r.w_part, r.w_from.at[0], (r.send_wt.at[0], r.recv_wt.at[0]), core_peer)

    def weight_x():
        return remote(r.w_half, r.w_from.at[1], (r.send_wt.at[1], r.recv_wt.at[1]), x_peer)

    def weight_ep(k):
        return remote(
            r.w_sum, r.w_back.at[me], (r.send_we.at[k], r.recv_we.at[k]), (src(k), t)
        )

    weight_core().start()
    tile(0, 0)
    sum_core(n_ep - 1)
    weight_core().wait_recv()
    r.w_half[...] = r.w_part[...] + r.w_from[0]
    send_back(n_ep - 2)
    weight_x().start()
    for j in range(1, tiles):
        tile(0, j)
    weight_x().wait_recv()
    r.w_sum[...] = r.w_half[...] + r.w_from[1]
    send_back(n_ep - 1)
    r.w_back[me] = r.w_sum[...]

    @pl.loop(1, n_ep)
    def _(k):
        weight_ep(k).start()

    for kind in (1, 2):
        for j in range(tiles):
            tile(kind, j)

    @pl.loop(1, n_ep)
    def _(k):
        grad_hop(k).wait_recv()
        gate_hop(k).wait_recv()

    total = jnp.zeros((2, own_rows, rank_r), F32)
    gate_total = jnp.zeros(r.gg_out.shape, F32)
    for e in range(n_ep):
        total = total + r.dg_back[e].astype(F32)
        gate_total = gate_total + r.gg_back[e]
    r.dg_out[...] = total
    r.gg_out[...] = gate_total

    @pl.loop(1, n_ep)
    def _(k):
        weight_ep(k).wait_recv()
        back_ep(k).wait_recv()

    picks = r.picks[...].reshape(rows, tok_dev)
    moved = lax.dot_general(
        picks,
        r.rows_back[...].reshape(rows, cols),
        CONTRACT_ROWS,
        preferred_element_type=F32,
    )
    r.grad_tokens[...] = (r.dense_dx[...] + moved).astype(BF)
    found = [jnp.zeros((1, tok_dev), F32) for _ in range(top_k)]
    for e in range(n_ep):
        row = r.w_back[e, pl.ds(me, 1), :]
        row = jnp.broadcast_to(row, (16, lanes)).astype(BF)[:, :cap]
        spread = jnp.dot(row, r.picks[e], preferred_element_type=F32)[0:1]
        for k in range(top_k):
            found[k] = found[k] + jnp.where(r.ids[k : k + 1, :] == e, spread, 0.0)
    for k in range(top_k):
        r.grad_route[k : k + 1, :] = found[k].astype(BF)

    @pl.loop(0, n_ep)
    def _(k):
        for kind in (1, 2, 3):
            shard_hop(kind, k).wait_send()
        for h in range(2):
            back_core(k, h).wait_send()
        back_x(k).wait_send()

    @pl.loop(1, n_ep)
    def _(k):
        shard_hop(0, k).wait_send()
        for a in range(2):
            for kind in range(4):
                row_hop(a, kind, k).wait_send()
        w_hop(k).wait_send()
        back_ep(k).wait_send()
        weight_ep(k).wait_send()
        grad_hop(k).wait_send()
        gate_hop(k).wait_send()

    weight_core().wait_send()
    weight_x().wait_send()
    for number in range(3 * tiles - stages, 3 * tiles):
        tile_out(number // tiles, number % tiles, number % stages).wait()


def shards(
    tokens,
    cotangent,
    route_ids,
    route_weights,
    w_gate,
    w_up,
    w_down,
    dense_in,
    dense_out,
    dense_gate,
):
    n_ep = lax.axis_size("ep")
    n_tp = lax.axis_size("tp")
    tok_dev, width = tokens.shape
    top_k = route_ids.shape[1]
    cols = width // n_tp
    cap = 2 * tok_dev * top_k // n_ep
    lanes = -(-cap // 128) * 128
    hidden = w_gate.shape[2]
    own_rows, rank_r = dense_in.shape
    gate_lanes = -(-(width // n_ep) // 128) * 128
    dma = pltpu.SemaphoreType.DMA
    stages = 3
    args = dict(
        ids=(route_ids.T, VMEM),
        route=(route_weights.T, VMEM),
        gate_row=(dense_gate[None], VMEM),
        tokens=(tokens, ANY),
        cotangent=(cotangent, ANY),
        in_own=(dense_in, ANY),
        out_own=(dense_out, ANY),
        w_gate=(w_gate[0], ANY),
        w_up=(w_up[0], ANY),
        w_down=(w_down[0], ANY),
    )
    outs = dict(
        grad_tokens=((tok_dev, cols), BF, VMEM),
        grad_route=((top_k, tok_dev), BF, VMEM),
        grad_gate=((width, hidden), F32, ANY),
        grad_up=((width, hidden), F32, ANY),
        grad_down=((hidden, width), F32, ANY),
        dg_out=((2, own_rows, rank_r), F32, VMEM),
        gg_out=((8, gate_lanes), F32, VMEM),
    )
    scratch = dict(
        tok=((tok_dev, width), BF),
        cot=((tok_dev, width), BF),
        gate_w=((width, hidden), BF),
        up_w=((width, hidden), BF),
        down_w=((hidden, width), BF),
        pos=((max(16, n_ep), tok_dev), F32),
        weight=((max(16, n_ep), tok_dev), F32),
        picks=((n_ep, cap, tok_dev), BF),
        w_send=((n_ep, 8, lanes), F32),
        w_all=((n_ep, 8, lanes), F32),
        x_send=((n_ep, cap, cols), BF),
        dy_send=((n_ep, cap, cols), BF),
        x_all=((n_ep, cap, width), BF),
        dy_all=((n_ep, cap, width), BF),
        scaled=((n_ep, cap, width), BF),
        act=((n_ep, cap, hidden), BF),
        d_gate=((n_ep, cap, hidden), BF),
        d_up=((n_ep, cap, hidden), BF),
        part=((n_ep, cap, width), BF),
        w_part=((n_ep, lanes), F32),
        from_core=((n_ep, 2, cap, cols), BF),
        to_x=((n_ep, cap, cols), BF),
        from_x=((n_ep, cap, cols), BF),
        to_ep=((n_ep, cap, cols), BF),
        rows_back=((n_ep, cap, cols), BF),
        dense_all=((n_ep, n_tp, 2, own_rows, rank_r), BF),
        dense_dx=((tok_dev, cols), F32),
        dense_grad=((width, rank_r), F32),
        dg_send=((n_ep, 2, own_rows, rank_r), BF),
        dg_back=((n_ep, 2, own_rows, rank_r), BF),
        gg_send=((n_ep, 8, gate_lanes), F32),
        gg_back=((n_ep, 8, gate_lanes), F32),
        w_from=((2, n_ep, lanes), F32),
        w_half=((n_ep, lanes), F32),
        w_sum=((n_ep, lanes), F32),
        w_back=((n_ep, n_ep, lanes), F32),
        stage=((stages, cols, hidden), F32),
    )
    sems = dict(
        load_sem=(7,),
        send_rows=(2, 4, n_ep),
        recv_rows=(2, 4, n_ep),
        send_shard=(4, n_ep),
        recv_shard=(4, n_ep),
        send_w=(n_ep,),
        recv_w=(n_ep,),
        send_bc=(n_ep, 2),
        recv_bc=(n_ep, 2),
        send_bx=(n_ep,),
        recv_bx=(n_ep,),
        send_be=(n_ep,),
        recv_be=(n_ep,),
        send_dg=(n_ep,),
        recv_dg=(n_ep,),
        send_gg=(n_ep,),
        recv_gg=(n_ep,),
        send_wt=(2,),
        recv_wt=(2,),
        send_we=(n_ep,),
        recv_we=(n_ep,),
        tile_sem=(3 * (width // cols),),
    )
    names = list(args) + list(outs) + list(scratch) + list(sems)
    results = pl.pallas_call(
        functools.partial(layer_kernel, n_ep, n_tp, names),
        out_shape=tuple(jax.ShapeDtypeStruct(s, d) for s, d, _ in outs.values()),
        in_specs=[spec for _, spec in args.values()],
        out_specs=tuple(spec for _, _, spec in outs.values()),
        scratch_shapes=[pltpu.VMEM(s, d) for s, d in scratch.values()]
        + [dma(s) for s in sems.values()],
        compiler_params=pltpu.CompilerParams(
            collective_id=0, has_side_effects=True, vmem_limit_bytes=63 * 1024 * 1024
        ),
        name="layer",
    )(*(a for a, _ in args.values()))
    grad_tokens, grad_route, grad_gate, grad_up, grad_down, dg_out, gg_out = results
    block = width // (n_ep * n_tp)
    grad_dense_gate = lax.dynamic_slice_in_dim(gg_out[0], lax.axis_index("tp") * block, block)
    return (
        grad_tokens,
        grad_route.T,
        grad_gate[None],
        grad_up[None],
        grad_down[None],
        dg_out[0],
        dg_out[1],
        grad_dense_gate,
    )


def solution(mesh):
    placed = (
        P("ep", None),
        P("ep", None),
        P("ep", None),
        P("ep", None),
        P("ep", None, "tp"),
        P("ep", None, "tp"),
        P("ep", "tp", None),
        P(("ep", "tp"), None),
        P(("ep", "tp"), None),
        P(),
    )
    return jax.shard_map(
        shards,
        mesh=mesh,
        in_specs=placed,
        out_specs=(
            P("ep", "tp"),
            P("ep", None),
            P("ep", None, "tp"),
            P("ep", None, "tp"),
            P("ep", "tp", None),
            P(("ep", "tp"), None),
            P(("ep", "tp"), None),
            P(("ep", "tp")),
        ),
        check_vma=False,
    )
```

```python
import functools
import types

import jax
import jax.numpy as jnp
from jax import lax
from jax.experimental import pallas as pl
from jax.experimental.pallas import tpu as pltpu
from jax.sharding import PartitionSpec as P

CLAMP_LIMIT = 7.0
SIG_SLOPE = 1.702
MESH = pl.DeviceIdType.MESH
ANY = pl.BlockSpec(memory_space=pl.ANY)
VMEM = pl.BlockSpec(memory_space=pltpu.VMEM)
CONTRACT_COLS = (((1,), (1,)), ((), ()))
CONTRACT_ROWS = (((0,), (0,)), ((), ()))
F32 = jnp.float32
BF = jnp.bfloat16


def layer_kernel(n_ep, n_tp, names, *refs):
    r = types.SimpleNamespace(**dict(zip(names, refs)))
    me = lax.axis_index("ep")
    t = lax.axis_index("tp")
    half = t // 2
    side = t % 2
    t_core = half * 2 + 1 - side
    t_x = (1 - half) * 2 + side
    cap, cols = r.x_send.shape[1:]
    tok_dev, width = r.tok.shape
    top_k = r.ids.shape[0]
    lanes = r.w_all.shape[2]
    core_peer = (me, t_core)
    x_peer = (me, t_x)
    log = n_ep.bit_length() - 1
    near = n_ep // 4

    def dst(k):
        out = me
        for b in range(log):
            bit = (k // (1 << b)) % 2
            out = out + bit * (1 << b) * (1 - 2 * ((me // (1 << b)) % 2))
        return out

    src = dst
    planes = n_ep // near
    z = me // near
    inner = ((z + 1) // 2) % 2

    def seq(n):
        p = n + near - 1
        f = p // near
        k = jnp.where((f >= 2) & (inner == 1), (5 - f) * near + p % near, p)
        k = jnp.where(n > n_ep - near, n - (n_ep - near), k)
        return jnp.where(n == 0, 0, k)

    def quarter(q):
        return pl.ds(pl.multiple_of(q * cols, cols), cols)

    def remote(source, target, sems, device):
        return pltpu.make_async_remote_copy(
            src_ref=source,
            dst_ref=target,
            send_sem=sems[0],
            recv_sem=sems[1],
            device_id=device,
            device_id_type=MESH,
        )

    loads = [
        pltpu.make_async_copy(a, b, r.load_sem.at[n])
        for n, (a, b) in enumerate(
            (
                (r.in_own, r.dense_all.at[me, t, 0]),
                (r.out_own, r.dense_all.at[me, t, 1]),
                (r.tokens, r.tok),
                (r.cotangent, r.cot),
                (r.w_gate, r.gate_w),
                (r.w_up, r.up_w),
                (r.w_down, r.down_w),
            )
        )
    ]
    for c in loads:
        c.start()

    r.w_all[...] = jnp.zeros(r.w_all.shape, F32)
    peers = [(dst(k), t) for k in range(1, n_ep)] + [core_peer, x_peer]
    barrier = pltpu.get_barrier_semaphore()
    for device in peers:
        pl.semaphore_signal(barrier, inc=1, device_id=device, device_id_type=MESH)

    experts = r.pos.shape[0]
    expert_row = lax.broadcasted_iota(jnp.int32, (experts, tok_dev), 0)
    below = lax.broadcasted_iota(jnp.int32, (tok_dev, tok_dev), 0) < lax.broadcasted_iota(
        jnp.int32, (tok_dev, tok_dev), 1
    )
    r.below[...] = jnp.where(below, 1.0, 0.0).astype(BF)

    def place(s, pos, weight):
        member = jnp.zeros((experts, tok_dev), F32)
        scale = jnp.zeros((experts, tok_dev), F32)
        for k in range(top_k):
            hit = r.ids_all[s, k : k + 1, :] == expert_row
            member = jnp.where(hit, 1.0, member)
            scale = jnp.where(hit, r.route_all[s, k : k + 1, :], scale)
        rank = jnp.dot(member.astype(BF), r.below[...], preferred_element_type=F32)
        pos[...] = jnp.where(member > 0.0, rank, -1.0)
        weight[...] = scale

    r.ids_all[z] = r.ids[...]
    r.route_all[z] = r.route[...].astype(F32)
    place(z, r.own_pos, r.own_weight)
    r.w_send[...] = jnp.zeros(r.w_send.shape, F32)

    pl.semaphore_wait(barrier, len(peers))

    rows_send = (r.x_send, r.dy_send)
    extra_send = (r.x_extra, r.dy_extra)
    rows_all = (r.x_all, r.dy_all)

    def shard_hop(kind, k):
        sems = (r.send_shard.at[kind, k], r.recv_shard.at[kind, k])
        if kind == 0:
            block = r.dense_all.at[me, t]
            return remote(block, block, sems, (dst(k), t))
        if kind >= 4:
            block = r.dense_all.at[dst(k - k % near), t if kind == 4 else t_x]
            return remote(block, block, sems, (dst(k % near), t))
        block = r.dense_all.at[src(k), t_x if kind == 3 else t]
        return remote(block, block, sems, x_peer if kind == 1 else core_peer)

    def row_hop(a, kind, k):
        i = src(k)
        sems = (r.send_rows.at[a, kind, k], r.recv_rows.at[a, kind, k])
        if kind == 0:
            c = k % near
            return remote(
                rows_send[a].at[k], rows_all[a].at[dst(k - c), :, quarter(t)], sems, (dst(c), t)
            )
        if kind == 4:
            return remote(
                extra_send[a].at[k],
                rows_all[a].at[me, :, quarter(t_x)],
                (r.send_rows.at[a, 1, k], r.recv_rows.at[a, 1, k]),
                (dst(k), t),
            )
        block = rows_all[a].at[i, :, quarter(t_x if kind == 3 else t)]
        return remote(block, block, sems, x_peer if kind == 1 else core_peer)

    def w_hop(k):
        c = k % near
        return remote(
            r.w_send.at[k],
            r.w_all.at[dst(k - c)],
            (r.send_w.at[k], r.recv_w.at[k]),
            (dst(c), t),
        )

    own_raw = (r.tok, r.cot)
    raw = (r.x_raw, r.dy_raw)

    def raw_hop(a, s, up, own=False):
        plane = z + 1 if up else z - 1
        source = own_raw[a].at[:, quarter(t)] if own else raw[a].at[s]
        return remote(
            source,
            raw[a].at[s],
            (r.send_raw.at[a, int(up), s], r.recv_raw.at[a, s]),
            (plane * near + me % near, t),
        )

    def each_raw(a, s, act):
        @pl.when((s < z) & (z < planes - 1))
        def _():
            act(raw_hop(a, s, True))

        @pl.when((s > z) & (z > 0))
        def _():
            act(raw_hop(a, s, False))

    def each_own(a, act):
        @pl.when(z < planes - 1)
        def _():
            act(raw_hop(a, z, True, True))

        @pl.when(z > 0)
        def _():
            act(raw_hop(a, z, False, True))

    def pass_on(a, f):
        s = dst(f * near) // near
        raw_hop(a, s, False).wait_recv()
        each_raw(a, s, lambda copy: copy.start())

    def info_hop(kind, f):
        array = (r.ids_all, r.route_all)[kind]
        return remote(
            array.at[z],
            array.at[z],
            (r.send_info.at[kind, f], r.recv_info.at[kind, f]),
            (dst(f * near), t),
        )

    for f in range(1, planes):
        for kind in range(2):
            info_hop(kind, f).start()
    loads[2].wait()
    each_own(0, lambda c: c.start())
    loads[3].wait()
    each_own(1, lambda c: c.start())
    loads[0].wait()
    loads[1].wait()
    shard_hop(1, 0).start()
    shard_hop(2, 0).start()

    for k in range(near, n_ep, near):
        shard_hop(0, k).start()
    for k in range(1, near):
        shard_hop(4, k).start()

    slot = lax.broadcasted_iota(jnp.int32, (cap, tok_dev), 0).astype(F32)

    def pick_of(pos, e):
        return jnp.where(slot == pos[pl.ds(e, 1), :], 1.0, 0.0).astype(BF)

    def pick_rows(pos, weight, e):
        pick = pick_of(pos, e)
        wide = jnp.broadcast_to(weight[pl.ds(e, 1), :], (16, tok_dev)).astype(BF)
        sent = lax.dot_general(wide, pick, CONTRACT_COLS, preferred_element_type=F32)
        return pick, sent[:1]

    def picked(pick, rows):
        return jnp.dot(pick, rows, preferred_element_type=F32).astype(BF)

    def pick_close(a, k, pos, rows):
        @pl.loop(1, near)
        def _(c):
            rows_send[a][k + c] = picked(pick_of(pos, dst(c)), rows())

    def send_close(a, k):
        @pl.loop(1, near)
        def _(c):
            row_hop(a, 0, k + c).start()

    def weigh_close(k, pos, weight):
        @pl.loop(1, near)
        def _(c):
            _, sent = pick_rows(pos, weight, dst(c))
            r.w_send[k + c, :, :cap] = sent
            w_hop(k + c).start()

    for a in range(2):
        pick_close(a, 0, r.own_pos, lambda: own_raw[a][:, quarter(t)])
    for a in range(2):
        send_close(a, 0)
    pick, sent = pick_rows(r.own_pos, r.own_weight, me)
    r.w_all[me, :, :cap] = sent
    weigh_close(0, r.own_pos, r.own_weight)

    @pl.loop(1, near)
    def _(c):
        extra, _ = pick_rows(r.own_pos, r.own_weight, dst(c))
        r.x_extra[c] = picked(extra, r.tok[:, quarter(t_x)])
        r.dy_extra[c] = picked(extra, r.cot[:, quarter(t_x)])

    @pl.loop(0, n_tp)
    def _(q):
        r.x_all[me, :, quarter(q)] = jnp.dot(
            pick, r.tok[:, quarter(q)], preferred_element_type=F32
        ).astype(BF)
        r.dy_all[me, :, quarter(q)] = jnp.dot(
            pick, r.cot[:, quarter(q)], preferred_element_type=F32
        ).astype(BF)

    @pl.loop(1, near)
    def _(c):
        for a in range(2):
            row_hop(a, 4, c).start()

    for c in loads[4:]:
        c.wait()

    diagonal = lax.broadcasted_iota(jnp.int32, (cap, lanes), 0) == lax.broadcasted_iota(
        jnp.int32, (cap, lanes), 1
    )

    def compute(i):
        weight_row = r.w_all[i]
        route_col = jnp.sum(jnp.where(diagonal, weight_row, 0.0), axis=1, keepdims=True)
        x_rows = r.x_all[i]
        gate_pre = jnp.dot(x_rows, r.gate_w[...], preferred_element_type=F32)
        up_pre = jnp.dot(x_rows, r.up_w[...], preferred_element_type=F32)
        gate_clamp = jnp.minimum(gate_pre, CLAMP_LIMIT)
        up_clamp = jnp.clip(up_pre, -CLAMP_LIMIT, CLAMP_LIMIT)
        sig = jax.nn.sigmoid(SIG_SLOPE * gate_clamp)
        act = (gate_clamp * sig * (up_clamp + 1.0)).astype(BF)
        act_wide = act.astype(F32)
        r.act[i] = (route_col * act_wide).astype(BF)
        dy_rows = r.dy_all[i]
        back = lax.dot_general(dy_rows, r.down_w[...], CONTRACT_COLS, preferred_element_type=F32)
        weight_sum = jnp.sum(act_wide * back, axis=1, keepdims=True)
        r.w_part[i] = jnp.sum(
            jnp.where(diagonal, weight_sum, 0.0), axis=0, keepdims=True
        )
        d_act = route_col * back
        d_gate = jnp.where(
            gate_pre < CLAMP_LIMIT,
            d_act * (up_clamp + 1.0) * (sig + SIG_SLOPE * gate_clamp * sig * (1.0 - sig)),
            0.0,
        ).astype(BF)
        d_up = jnp.where(jnp.abs(up_pre) < CLAMP_LIMIT, d_act * gate_clamp * sig, 0.0).astype(BF)
        r.d_gate[i] = d_gate
        r.d_up[i] = d_up
        part = lax.dot_general(d_gate, r.gate_w[...], CONTRACT_COLS, preferred_element_type=F32)
        part = part + lax.dot_general(
            d_up, r.up_w[...], CONTRACT_COLS, preferred_element_type=F32
        )
        r.part[i] = part.astype(BF)

    def back_core(k, h):
        return remote(
            r.part.at[src(k), :, quarter(h * 2 + 1 - side)],
            r.from_core.at[k, h],
            (r.send_bc.at[k, h], r.recv_bc.at[k, h]),
            core_peer,
        )

    def back_x(k):
        return remote(
            r.part.at[src(k), :, quarter(t_x)],
            r.from_x.at[k],
            (r.send_bx.at[k], r.recv_bx.at[k]),
            x_peer,
        )

    def back_ep(k):
        return remote(
            r.part.at[src(k), :, quarter(t)],
            r.rows_back.at[me],
            (r.send_be.at[k], r.recv_be.at[k]),
            (src(k), t),
        )

    def run(k):
        compute(src(k))
        for h in range(2):
            back_core(k, h).start()

    def sum_core(k):
        for h in range(2):
            back_core(k, h).wait_recv()
        other = r.part[src(k), :, quarter(t_x)].astype(F32)
        other = other + r.from_core[k, 1 - half].astype(F32)
        r.part[src(k), :, quarter(t_x)] = other.astype(BF)
        back_x(k).start()

    def sum_x(k):
        back_x(k).wait_recv()
        mine = r.part[src(k), :, quarter(t)].astype(F32)
        mine = mine + r.from_core[k, half].astype(F32)
        return (mine + r.from_x[k].astype(F32)).astype(BF)

    def send_back(k):
        r.part[src(k), :, quarter(t)] = sum_x(k)
        back_ep(k).start()

    def grad_near(k):
        return remote(
            r.dg_send.at[dst(k)],
            r.dg_near.at[k],
            (r.send_dg.at[k], r.recv_dg.at[k]),
            (dst(k % near), t),
        )

    def grad_far(k):
        return remote(
            r.dg_send.at[dst(k)], r.dg_far.at[k], (r.send_dg.at[k], r.recv_dg.at[k]), (dst(k), t)
        )

    close = [k for k in range(n_ep) if k % near]
    far = list(range(near, n_ep, near))

    def grad_sum():
        for k in close:
            grad_near(k).wait_recv()
        for f in [0] + far:
            total = r.dg_send[dst(f)].astype(F32)
            for k in range(f + 1, f + near):
                total = total + r.dg_near[k].astype(F32)
            if f:
                r.dg_send[dst(f)] = total.astype(BF)
                grad_far(f).start()
            else:
                r.dg_in[...] = total[0]
                r.dg_out[...] = total[1]

    def gate_hop(k):
        return remote(
            r.gg_send.at[dst(k)], r.gg_back.at[me], (r.send_gg.at[k], r.recv_gg.at[k]), (dst(k), t)
        )

    own_rows, rank_r = r.in_own.shape
    span = n_ep // n_tp
    block_cols = width // n_ep

    def dense():
        in_whole = r.dense_all[:, :, 0].reshape(width, rank_r)
        out_whole = r.dense_all[:, :, 1].reshape(width, rank_r)
        pre = jnp.dot(r.tok[...], in_whole, preferred_element_type=F32)
        cob = jnp.dot(r.cot[...], out_whole, preferred_element_type=F32)
        gate = r.gate_row[...].astype(F32)
        gate = jnp.concatenate([gate[j : j + 1] for j in range(width // 128)], axis=1)
        r.gate_f32[...] = gate
        gate_wide = jnp.broadcast_to(gate, (16, width)).astype(BF)
        logit = lax.dot_general(
            r.tok[...], gate_wide, CONTRACT_COLS, preferred_element_type=F32
        )[:, :1]
        mix = jax.nn.sigmoid(logit)
        sig = jax.nn.sigmoid(pre)
        act = (pre * sig).astype(BF)
        dpre = (mix * cob * sig * (1.0 + pre * (1.0 - sig))).astype(BF)
        act_wide = act.astype(F32)
        dlogit = mix * (1.0 - mix) * jnp.sum(act_wide * cob, axis=1, keepdims=True)
        in_rows = r.dense_all[pl.ds(t * span, span), :, 0].reshape(cols, rank_r)
        dx = lax.dot_general(dpre, in_rows, CONTRACT_COLS, preferred_element_type=F32)
        r.dense_dx[...] = dx + dlogit * r.gate_f32[:, quarter(t)]
        lane = lax.broadcasted_iota(jnp.int32, (tok_dev, 128), 1)
        high = dlogit.astype(BF).astype(F32)
        low = dlogit - high
        pair = jnp.where(lane == 0, high, jnp.where(lane == 1, low, 0.0)).astype(BF)
        gate_sum = lax.dot_general(pair, r.tok[...], CONTRACT_ROWS, preferred_element_type=F32)
        gate_sum = gate_sum[0:1] + gate_sum[1:2]
        for e in range(n_ep):
            r.gg_send[e, :, :block_cols] = gate_sum[:, e * block_cols : (e + 1) * block_cols]
        mixed = (mix * act_wide).astype(BF)
        for a, (left, right) in enumerate(((r.tok, dpre), (r.cot, mixed))):
            r.grad_gate[:, :rank_r] = lax.dot_general(
                left[...], right, CONTRACT_ROWS, preferred_element_type=F32
            )
            for e in range(n_ep):
                start = pl.multiple_of((e * n_tp + t) * own_rows, own_rows)
                r.dg_send[e, a] = r.grad_gate[
                    pl.ds(start, own_rows), :rank_r
                ].astype(BF)
        r.gg_back[me] = r.gg_send[me]

        @pl.loop(1, n_ep)
        def _(k):
            gate_hop(k).start()

        for k in close:
            grad_near(k).start()

    @pl.loop(0, n_ep + 2)
    def _(n):
        @pl.when(n == 1)
        def _():
            sum_core(0)

        @pl.when(n == 3)
        def _():
            for f in far:
                shard_hop(0, f).wait_recv()
                shard_hop(1, f).start()
                shard_hop(2, f).start()
                for k in range(f + 1, f + near):
                    shard_hop(4, k).start()

        @pl.when((n >= 1) & (n < n_ep))
        def _():
            k = seq(n)
            c = k % near

            @pl.when(c > 0)
            def _():
                for a in range(2):
                    row_hop(a, 0, k).wait_recv()

                    @pl.when(k >= near)
                    def _():
                        row_hop(a, 1, k).start()

                    row_hop(a, 2, k).start()
                w_hop(k).wait_recv()

            @pl.when(c == 0)
            def _():
                i = src(k)
                s = i // near
                for kind in range(2):
                    info_hop(kind, k // near).wait_recv()
                place(s, r.pos, r.weight)
                pick, sent = pick_rows(r.pos, r.weight, me)
                r.w_all[i, :, :cap] = sent
                for a in range(2):

                    @pl.when((inner == 1) & (n == 1))
                    def _():
                        pass_on(a, 1)
                        pass_on(a, 3)

                    @pl.when(inner == 0)
                    def _():
                        raw_hop(a, s, False).wait_recv()

                    rows_all[a][i, :, quarter(t)] = picked(pick, raw[a][s])
                    pick_close(a, k, r.pos, lambda: raw[a][s])
                    row_hop(a, 1, k).start()
                    row_hop(a, 2, k).start()
                    send_close(a, k)

                weigh_close(k, r.pos, r.weight)

        @pl.when(n >= 4)
        def _():
            sum_core(seq(n - 3))

        @pl.when(n == 3)
        def _():
            r.rows_back[me] = sum_x(0)

        @pl.when(n >= 5)
        def _():
            send_back(seq(n - 4))

        @pl.when((n == 0) | (n >= 3))
        def _():
            k = seq(jnp.where(n == 0, 0, n - 2))

            @pl.when(n >= 3)
            def _():
                for a in range(2):
                    for kind in (2, 3):
                        row_hop(a, kind, k).wait_recv()

            run(k)

        @pl.when(n == 0)
        def _():
            @pl.loop(0, n_ep)
            def _(e):
                pick, _ = pick_rows(r.own_pos, r.own_weight, e)
                r.picks[e] = pick

        @pl.when(n == 4)
        def _():
            for f in [0] + far:
                shard_hop(1, f).wait_recv()
                shard_hop(3, f).start()
                for k in range(f + 1, f + near):
                    shard_hop(5, k).start()

        @pl.when(n == 5)
        def _():
            for k in close:
                shard_hop(4, k).wait_recv()
                shard_hop(2, k).start()
                shard_hop(5, k).wait_recv()
                shard_hop(3, k).start()

        @pl.when((n >= 2) & (n < n_ep + 1))
        def _():
            k = seq(n - 1)
            for a in range(2):
                row_hop(a, 1, k).wait_recv()
                row_hop(a, 3, k).start()

        @pl.when(n == 7)
        def _():
            grad_sum()

        @pl.when((inner == 1) & (n == near + 1))
        def _():
            for a in range(2):
                pass_on(a, 2)

        @pl.when(n == 6)
        def _():
            @pl.loop(0, n_ep)
            def _(k):
                for kind in (2, 3):
                    shard_hop(kind, k).wait_recv()

            dense()

    rows = n_ep * cap
    tiles = width // cols

    def tile(kind, j):
        if kind == 0:
            r.grad_down[:, quarter(j)] = lax.dot_general(
                r.act[...].reshape(rows, -1),
                r.dy_all.reshape(rows, width)[:, quarter(j)],
                CONTRACT_ROWS,
                preferred_element_type=F32,
            )
            return
        out, right = ((r.grad_gate, r.d_gate), (r.grad_up, r.d_up))[kind - 1]
        out[quarter(j), :] = lax.dot_general(
            r.x_all.reshape(rows, width)[:, quarter(j)],
            right[...].reshape(rows, -1),
            CONTRACT_ROWS,
            preferred_element_type=F32,
        )

    def weight_core():
        return remote(r.w_part, r.w_from.at[0], (r.send_wt.at[0], r.recv_wt.at[0]), core_peer)

    def weight_x():
        return remote(r.w_half, r.w_from.at[1], (r.send_wt.at[1], r.recv_wt.at[1]), x_peer)

    def weight_ep(k):
        return remote(
            r.w_sum.at[src(k)], r.w_back.at[me], (r.send_we.at[k], r.recv_we.at[k]), (src(k), t)
        )

    weight_core().start()
    tile(0, 0)
    sum_core(seq(n_ep - 1))
    weight_core().wait_recv()
    r.w_half[...] = r.w_part[...] + r.w_from[0]
    send_back(seq(n_ep - 2))
    weight_x().start()
    for j in range(1, tiles):
        tile(0, j)
    weight_x().wait_recv()
    r.w_sum[...] = r.w_half[...] + r.w_from[1]
    send_back(seq(n_ep - 1))
    r.w_back[me] = r.w_sum[me]

    @pl.loop(1, n_ep)
    def _(k):
        weight_ep(k).start()

    for kind in (1, 2):
        for j in range(tiles):
            tile(kind, j)

    @pl.loop(1, n_ep)
    def _(k):
        gate_hop(k).wait_recv()

    for f in far:
        grad_far(f).wait_recv()
        r.dg_in[...] += r.dg_far[f, 0].astype(F32)
        r.dg_out[...] += r.dg_far[f, 1].astype(F32)
    gate_total = jnp.zeros(r.gg_back.shape[1:], F32)
    for e in range(n_ep):
        gate_total = gate_total + r.gg_back[e]
    block = block_cols // n_tp
    r.gg_out[...] = sum(
        jnp.where(t == q, gate_total[:, q * block : (q + 1) * block], 0.0) for q in range(n_tp)
    )

    @pl.loop(1, n_ep)
    def _(k):
        weight_ep(k).wait_recv()
        back_ep(k).wait_recv()

    picks = r.picks[...].reshape(rows, tok_dev)
    moved = lax.dot_general(
        picks,
        r.rows_back[...].reshape(rows, cols),
        CONTRACT_ROWS,
        preferred_element_type=F32,
    )
    r.grad_tokens[...] = (r.dense_dx[...] + moved).astype(BF)
    found = [jnp.zeros((1, tok_dev), F32) for _ in range(top_k)]
    for e in range(n_ep):
        row = r.w_back[e]
        row = jnp.broadcast_to(row, (16, lanes)).astype(BF)[:, :cap]
        spread = jnp.dot(row, r.picks[e], preferred_element_type=F32)[0:1]
        for k in range(top_k):
            found[k] = found[k] + jnp.where(r.ids[k : k + 1, :] == e, spread, 0.0)
    for k in range(top_k):
        r.grad_route[k : k + 1, :] = found[k].astype(BF)

    for f in [0] + far:
        shard_hop(1, f).wait_send()
    for f in far:
        shard_hop(0, f).wait_send()
        grad_far(f).wait_send()
    for f in range(1, planes):
        for kind in range(2):
            info_hop(kind, f).wait_send()
    for a in range(2):
        each_own(a, lambda c: c.wait_send())
        for s in range(planes):
            each_raw(a, s, lambda c: c.wait_send())
    for k in close:
        w_hop(k).wait_send()
        for a in range(2):
            row_hop(a, 0, k).wait_send()
        shard_hop(4, k).wait_send()
        shard_hop(5, k).wait_send()
        grad_near(k).wait_send()

    @pl.loop(0, n_ep)
    def _(k):
        for kind in (2, 3):
            shard_hop(kind, k).wait_send()
        for h in range(2):
            back_core(k, h).wait_send()
        back_x(k).wait_send()

    @pl.loop(1, n_ep)
    def _(k):
        for a in range(2):
            for kind in range(1, 4):
                row_hop(a, kind, k).wait_send()
        back_ep(k).wait_send()
        weight_ep(k).wait_send()
        gate_hop(k).wait_send()

    weight_core().wait_send()
    weight_x().wait_send()


def store_kernel(count, *refs):
    copies = [
        pltpu.make_async_copy(refs[n], refs[count + n], refs[2 * count].at[n])
        for n in range(count)
    ]
    for c in copies:
        c.start()
    for c in copies:
        c.wait()


def store(arrays):
    return pl.pallas_call(
        functools.partial(store_kernel, len(arrays)),
        out_shape=tuple(jax.ShapeDtypeStruct(a.shape, a.dtype) for a in arrays),
        in_specs=[VMEM] * len(arrays),
        out_specs=(ANY,) * len(arrays),
        scratch_shapes=[pltpu.SemaphoreType.DMA((len(arrays),))],
        compiler_params=pltpu.CompilerParams(vmem_limit_bytes=16 * 1024 * 1024),
        name="store",
    )(*arrays)


def shards(
    tokens,
    cotangent,
    route_ids,
    route_weights,
    w_gate,
    w_up,
    w_down,
    dense_in,
    dense_out,
    dense_gate,
):
    n_ep = lax.axis_size("ep")
    n_tp = lax.axis_size("tp")
    tok_dev, width = tokens.shape
    top_k = route_ids.shape[1]
    cols = width // n_tp
    near = n_ep // 4
    cap = 2 * tok_dev * top_k // n_ep
    lanes = -(-cap // 128) * 128
    hidden = w_gate.shape[2]
    own_rows, rank_r = dense_in.shape
    gate_lanes = -(-(width // n_ep) // 128) * 128
    dma = pltpu.SemaphoreType.DMA
    args = dict(
        ids=(route_ids.T, VMEM),
        route=(route_weights.T, VMEM),
        gate_row=(dense_gate.reshape(-1, 128), VMEM),
        tokens=(tokens, ANY),
        cotangent=(cotangent, ANY),
        in_own=(dense_in, ANY),
        out_own=(dense_out, ANY),
        w_gate=(w_gate[0], ANY),
        w_up=(w_up[0], ANY),
        w_down=(w_down[0], ANY),
    )
    outs = dict(
        grad_tokens=((tok_dev, cols), BF),
        grad_route=((top_k, tok_dev), BF),
        grad_gate=((width, hidden), F32),
        grad_up=((width, hidden), F32),
        grad_down=((hidden, width), F32),
        dg_in=((own_rows, rank_r), F32),
        dg_out=((own_rows, rank_r), F32),
        gg_out=((1, width // (n_ep * n_tp)), F32),
    )
    scratch = dict(
        tok=((tok_dev, width), BF),
        cot=((tok_dev, width), BF),
        gate_w=((width, hidden), BF),
        up_w=((width, hidden), BF),
        down_w=((hidden, width), BF),
        own_pos=((max(16, n_ep), tok_dev), F32),
        own_weight=((max(16, n_ep), tok_dev), F32),
        pos=((max(16, n_ep), tok_dev), F32),
        weight=((max(16, n_ep), tok_dev), F32),
        below=((tok_dev, tok_dev), BF),
        ids_all=((4, top_k, tok_dev), jnp.int32),
        route_all=((4, top_k, tok_dev), F32),
        x_extra=((near, cap, cols), BF),
        dy_extra=((near, cap, cols), BF),
        x_raw=((4, tok_dev, cols), BF),
        dy_raw=((4, tok_dev, cols), BF),
        picks=((n_ep, cap, tok_dev), BF),
        w_send=((n_ep, 1, lanes), F32),
        w_all=((n_ep, 1, lanes), F32),
        x_send=((n_ep, cap, cols), BF),
        dy_send=((n_ep, cap, cols), BF),
        x_all=((n_ep, cap, width), BF),
        dy_all=((n_ep, cap, width), BF),
        act=((n_ep, cap, hidden), BF),
        d_gate=((n_ep, cap, hidden), BF),
        d_up=((n_ep, cap, hidden), BF),
        part=((n_ep, cap, width), BF),
        w_part=((n_ep, 1, lanes), F32),
        from_core=((n_ep, 2, cap, cols), BF),
        from_x=((n_ep, cap, cols), BF),
        rows_back=((n_ep, cap, cols), BF),
        dense_all=((n_ep, n_tp, 2, own_rows, rank_r), BF),
        dense_dx=((tok_dev, cols), F32),
        gate_f32=((1, width), F32),
        dg_send=((n_ep, 2, own_rows, rank_r), BF),
        dg_near=((n_ep, 2, own_rows, rank_r), BF),
        dg_far=((n_ep, 2, own_rows, rank_r), BF),
        gg_send=((n_ep, 1, gate_lanes), F32),
        gg_back=((n_ep, 1, gate_lanes), F32),
        w_from=((2, n_ep, 1, lanes), F32),
        w_half=((n_ep, 1, lanes), F32),
        w_sum=((n_ep, 1, lanes), F32),
        w_back=((n_ep, 1, lanes), F32),
    )
    sems = dict(
        load_sem=(7,),
        send_info=(2, 4),
        recv_info=(2, 4),
        send_raw=(2, 2, 4),
        recv_raw=(2, 4),
        send_rows=(2, 4, n_ep),
        recv_rows=(2, 4, n_ep),
        send_shard=(6, n_ep),
        recv_shard=(6, n_ep),
        send_w=(n_ep,),
        recv_w=(n_ep,),
        send_bc=(n_ep, 2),
        recv_bc=(n_ep, 2),
        send_bx=(n_ep,),
        recv_bx=(n_ep,),
        send_be=(n_ep,),
        recv_be=(n_ep,),
        send_dg=(n_ep,),
        recv_dg=(n_ep,),
        send_gg=(n_ep,),
        recv_gg=(n_ep,),
        send_wt=(2,),
        recv_wt=(2,),
        send_we=(n_ep,),
        recv_we=(n_ep,),
    )
    names = list(args) + list(outs) + list(scratch) + list(sems)
    results = pl.pallas_call(
        functools.partial(layer_kernel, n_ep, n_tp, names),
        out_shape=tuple(pltpu.VMEM(s, d) for s, d in outs.values()),
        in_specs=[spec for _, spec in args.values()],
        out_specs=(VMEM,) * len(outs),
        scratch_shapes=[pltpu.VMEM(s, d) for s, d in scratch.values()]
        + [dma(s) for s in sems.values()],
        compiler_params=pltpu.CompilerParams(
            collective_id=0, has_side_effects=True, vmem_limit_bytes=48 * 1024 * 1024
        ),
        name="layer",
    )(*(a for a, _ in args.values()))
    grad_tokens, grad_route, grad_gate, grad_up, grad_down, dg_in, dg_out, gg_out = store(results)
    return (
        grad_tokens,
        grad_route.T,
        grad_gate[None],
        grad_up[None],
        grad_down[None],
        dg_in,
        dg_out,
        gg_out[0],
    )


def solution(mesh):
    placed = (
        P("ep", None),
        P("ep", None),
        P("ep", None),
        P("ep", None),
        P("ep", None, "tp"),
        P("ep", None, "tp"),
        P("ep", "tp", None),
        P(("ep", "tp"), None),
        P(("ep", "tp"), None),
        P(),
    )
    return jax.shard_map(
        shards,
        mesh=mesh,
        in_specs=placed,
        out_specs=(
            P("ep", "tp"),
            P("ep", None),
            P("ep", None, "tp"),
            P("ep", None, "tp"),
            P("ep", "tp", None),
            P(("ep", "tp"), None),
            P(("ep", "tp"), None),
            P(("ep", "tp")),
        ),
        check_vma=False,
    )
```

```python
import functools
import types

import jax
import jax.numpy as jnp
from jax import lax
from jax.experimental import pallas as pl
from jax.experimental.pallas import tpu as pltpu
from jax.sharding import PartitionSpec as P

CLAMP_LIMIT = 7.0
SIG_SLOPE = 1.702
MESH = pl.DeviceIdType.MESH
ANY = pl.BlockSpec(memory_space=pl.ANY)
VMEM = pl.BlockSpec(memory_space=pltpu.VMEM)
CONTRACT_COLS = (((1,), (1,)), ((), ()))
CONTRACT_ROWS = (((0,), (0,)), ((), ()))
F32 = jnp.float32
BF = jnp.bfloat16


def layer_kernel(n_ep, n_tp, names, *refs):
    r = types.SimpleNamespace(**dict(zip(names, refs)))
    me = lax.axis_index("ep")
    t = lax.axis_index("tp")
    half = t // 2
    side = t % 2
    t_core = half * 2 + 1 - side
    t_x = (1 - half) * 2 + side
    cap, cols = r.x_send.shape[1:]
    tok_dev, width = r.tok.shape
    top_k = r.ids.shape[0]
    lanes = r.w_all.shape[2]
    core_peer = (me, t_core)
    x_peer = (me, t_x)
    log = n_ep.bit_length() - 1
    near = n_ep // 4

    def dst(k):
        out = me
        for b in range(log):
            bit = (k // (1 << b)) % 2
            out = out + bit * (1 << b) * (1 - 2 * ((me // (1 << b)) % 2))
        return out

    src = dst
    planes = n_ep // near
    z = me // near
    inner = ((z + 1) // 2) % 2

    def seq(n):
        p = n + near - 1
        f = p // near
        k = jnp.where(inner == 1, ((f + 1) % 3 + 1) * near + p % near, p)
        k = jnp.where(n > n_ep - near, n - (n_ep - near), k)
        return jnp.where(n == 0, 0, k)

    def quarter(q):
        return pl.ds(pl.multiple_of(q * cols, cols), cols)

    def remote(source, target, sems, device):
        return pltpu.make_async_remote_copy(
            src_ref=source,
            dst_ref=target,
            send_sem=sems[0],
            recv_sem=sems[1],
            device_id=device,
            device_id_type=MESH,
        )

    loads = [
        pltpu.make_async_copy(a, b, r.load_sem.at[n])
        for n, (a, b) in enumerate(
            (
                (r.in_own, r.dense_all.at[me, t, 0]),
                (r.out_own, r.dense_all.at[me, t, 1]),
                (r.tokens, r.tok),
                (r.cotangent, r.cot),
                (r.w_gate, r.gate_w),
                (r.w_up, r.up_w),
                (r.w_down, r.down_w),
            )
        )
    ]
    for c in loads:
        c.start()

    r.w_all[...] = jnp.zeros(r.w_all.shape, F32)
    peers = [(dst(k), t) for k in range(1, n_ep)] + [core_peer, x_peer]
    barrier = pltpu.get_barrier_semaphore()
    for device in peers:
        pl.semaphore_signal(barrier, inc=1, device_id=device, device_id_type=MESH)

    experts = r.pos.shape[0]
    expert_row = lax.broadcasted_iota(jnp.int32, (experts, tok_dev), 0)
    below = lax.broadcasted_iota(jnp.int32, (tok_dev, tok_dev), 0) < lax.broadcasted_iota(
        jnp.int32, (tok_dev, tok_dev), 1
    )
    r.below[...] = jnp.where(below, 1.0, 0.0).astype(BF)

    def place(s, pos, weight):
        member = jnp.zeros((experts, tok_dev), F32)
        scale = jnp.zeros((experts, tok_dev), F32)
        for k in range(top_k):
            hit = r.ids_all[s, k : k + 1, :] == expert_row
            member = jnp.where(hit, 1.0, member)
            scale = jnp.where(hit, r.route_all[s, k : k + 1, :], scale)
        rank = jnp.dot(member.astype(BF), r.below[...], preferred_element_type=F32)
        pos[...] = jnp.where(member > 0.0, rank, -1.0)
        weight[...] = scale

    r.ids_all[z] = r.ids[...]
    r.route_all[z] = r.route[...].astype(F32)
    place(z, r.own_pos, r.own_weight)
    r.w_send[...] = jnp.zeros(r.w_send.shape, F32)

    pl.semaphore_wait(barrier, len(peers))

    rows_send = (r.x_send, r.dy_send)
    extra_send = (r.x_extra, r.dy_extra)
    rows_all = (r.x_all, r.dy_all)

    def shard_hop(kind, k):
        sems = (r.send_shard.at[kind, k], r.recv_shard.at[kind, k])
        if kind == 0:
            block = r.dense_all.at[me, t]
            return remote(block, block, sems, (dst(k), t))
        if kind >= 4:
            block = r.dense_all.at[dst(k - k % near), t if kind == 4 else t_x]
            return remote(block, block, sems, (dst(k % near), t))
        block = r.dense_all.at[src(k), t_x if kind == 3 else t]
        return remote(block, block, sems, x_peer if kind == 1 else core_peer)

    def row_hop(a, kind, k):
        i = src(k)
        sems = (r.send_rows.at[a, kind, k], r.recv_rows.at[a, kind, k])
        if kind == 0:
            c = k % near
            return remote(
                rows_send[a].at[k], rows_all[a].at[dst(k - c), :, quarter(t)], sems, (dst(c), t)
            )
        if kind == 4:
            return remote(
                extra_send[a].at[k],
                rows_all[a].at[me, :, quarter(t_x)],
                (r.send_rows.at[a, 1, k], r.recv_rows.at[a, 1, k]),
                (dst(k), t),
            )
        block = rows_all[a].at[i, :, quarter(t_x if kind == 3 else t)]
        return remote(block, block, sems, x_peer if kind == 1 else core_peer)

    def w_hop(k):
        c = k % near
        return remote(
            r.w_send.at[k],
            r.w_all.at[dst(k - c)],
            (r.send_w.at[k], r.recv_w.at[k]),
            (dst(c), t),
        )

    own_raw = (r.tok, r.cot)
    raw = (r.x_raw, r.dy_raw)

    def raw_hop(a, s, up, own=False):
        plane = z + 1 if up else z - 1
        source = own_raw[a].at[:, quarter(t)] if own else raw[a].at[s]
        return remote(
            source,
            raw[a].at[s],
            (r.send_raw.at[a, int(up), s], r.recv_raw.at[a, s]),
            (plane * near + me % near, t),
        )

    def each_raw(a, s, act):
        @pl.when((s < z) & (z < planes - 1))
        def _():
            act(raw_hop(a, s, True))

        @pl.when((s > z) & (z > 0))
        def _():
            act(raw_hop(a, s, False))

    def each_own(a, act):
        @pl.when(z < planes - 1)
        def _():
            act(raw_hop(a, z, True, True))

        @pl.when(z > 0)
        def _():
            act(raw_hop(a, z, False, True))

    def pass_on(a, f):
        s = dst(f * near) // near
        raw_hop(a, s, False).wait_recv()
        each_raw(a, s, lambda copy: copy.start())

    def info_hop(kind, f):
        array = (r.ids_all, r.route_all)[kind]
        return remote(
            array.at[z],
            array.at[z],
            (r.send_info.at[kind, f], r.recv_info.at[kind, f]),
            (dst(f * near), t),
        )

    for f in range(1, planes):
        for kind in range(2):
            info_hop(kind, f).start()
    loads[2].wait()
    each_own(0, lambda c: c.start())
    loads[3].wait()
    each_own(1, lambda c: c.start())
    loads[0].wait()
    loads[1].wait()
    shard_hop(1, 0).start()
    shard_hop(2, 0).start()

    for k in range(near, n_ep, near):
        shard_hop(0, k).start()
    for k in range(1, near):
        shard_hop(4, k).start()

    slot = lax.broadcasted_iota(jnp.int32, (cap, tok_dev), 0).astype(F32)

    def pick_of(pos, e):
        return jnp.where(slot == pos[pl.ds(e, 1), :], 1.0, 0.0).astype(BF)

    def pick_rows(pos, weight, e):
        pick = pick_of(pos, e)
        wide = jnp.broadcast_to(weight[pl.ds(e, 1), :], (16, tok_dev)).astype(BF)
        sent = lax.dot_general(wide, pick, CONTRACT_COLS, preferred_element_type=F32)
        return pick, sent[:1]

    def picked(pick, rows):
        return jnp.dot(pick, rows, preferred_element_type=F32).astype(BF)

    def pick_close(a, k, pos, rows):
        @pl.loop(1, near)
        def _(c):
            rows_send[a][k + c] = picked(pick_of(pos, dst(c)), rows())

    def send_close(a, k):
        @pl.loop(1, near)
        def _(c):
            row_hop(a, 0, k + c).start()

    def weigh_close(k, pos, weight):
        @pl.loop(1, near)
        def _(c):
            _, sent = pick_rows(pos, weight, dst(c))
            r.w_send[k + c, :, :cap] = sent
            w_hop(k + c).start()

    for a in range(2):
        pick_close(a, 0, r.own_pos, lambda: own_raw[a][:, quarter(t)])
    for a in range(2):
        send_close(a, 0)
    pick, sent = pick_rows(r.own_pos, r.own_weight, me)
    r.w_all[me, :, :cap] = sent
    weigh_close(0, r.own_pos, r.own_weight)

    @pl.loop(1, near)
    def _(c):
        extra, _ = pick_rows(r.own_pos, r.own_weight, dst(c))
        r.x_extra[c] = picked(extra, r.tok[:, quarter(t_x)])
        r.dy_extra[c] = picked(extra, r.cot[:, quarter(t_x)])

    @pl.loop(0, n_tp)
    def _(q):
        r.x_all[me, :, quarter(q)] = jnp.dot(
            pick, r.tok[:, quarter(q)], preferred_element_type=F32
        ).astype(BF)
        r.dy_all[me, :, quarter(q)] = jnp.dot(
            pick, r.cot[:, quarter(q)], preferred_element_type=F32
        ).astype(BF)

    @pl.loop(1, near)
    def _(c):
        for a in range(2):
            row_hop(a, 4, c).start()

    for c in loads[4:]:
        c.wait()

    diagonal = lax.broadcasted_iota(jnp.int32, (cap, lanes), 0) == lax.broadcasted_iota(
        jnp.int32, (cap, lanes), 1
    )

    def compute(i):
        weight_row = r.w_all[i]
        route_col = jnp.sum(jnp.where(diagonal, weight_row, 0.0), axis=1, keepdims=True)
        x_rows = r.x_all[i]
        gate_pre = jnp.dot(x_rows, r.gate_w[...], preferred_element_type=F32)
        up_pre = jnp.dot(x_rows, r.up_w[...], preferred_element_type=F32)
        gate_clamp = jnp.minimum(gate_pre, CLAMP_LIMIT)
        up_clamp = jnp.clip(up_pre, -CLAMP_LIMIT, CLAMP_LIMIT)
        sig = jax.nn.sigmoid(SIG_SLOPE * gate_clamp)
        act = (gate_clamp * sig * (up_clamp + 1.0)).astype(BF)
        act_wide = act.astype(F32)
        r.act[i] = (route_col * act_wide).astype(BF)
        dy_rows = r.dy_all[i]
        back = lax.dot_general(dy_rows, r.down_w[...], CONTRACT_COLS, preferred_element_type=F32)
        weight_sum = jnp.sum(act_wide * back, axis=1, keepdims=True)
        r.w_part[i] = jnp.sum(
            jnp.where(diagonal, weight_sum, 0.0), axis=0, keepdims=True
        )
        d_act = route_col * back
        d_gate = jnp.where(
            gate_pre < CLAMP_LIMIT,
            d_act * (up_clamp + 1.0) * (sig + SIG_SLOPE * gate_clamp * sig * (1.0 - sig)),
            0.0,
        ).astype(BF)
        d_up = jnp.where(jnp.abs(up_pre) < CLAMP_LIMIT, d_act * gate_clamp * sig, 0.0).astype(BF)
        r.d_gate[i] = d_gate
        r.d_up[i] = d_up
        part = lax.dot_general(d_gate, r.gate_w[...], CONTRACT_COLS, preferred_element_type=F32)
        part = part + lax.dot_general(
            d_up, r.up_w[...], CONTRACT_COLS, preferred_element_type=F32
        )
        r.part[i] = part.astype(BF)

    def back_core(k, h):
        return remote(
            r.part.at[src(k), :, quarter(h * 2 + 1 - side)],
            r.from_core.at[k, h],
            (r.send_bc.at[k, h], r.recv_bc.at[k, h]),
            core_peer,
        )

    def back_x(k):
        return remote(
            r.part.at[src(k), :, quarter(t_x)],
            r.from_x.at[k],
            (r.send_bx.at[k], r.recv_bx.at[k]),
            x_peer,
        )

    def back_ep(k):
        return remote(
            r.part.at[src(k), :, quarter(t)],
            r.rows_back.at[me],
            (r.send_be.at[k], r.recv_be.at[k]),
            (src(k), t),
        )

    def run(k):
        compute(src(k))
        for h in range(2):
            back_core(k, h).start()

    def sum_core(k):
        for h in range(2):
            back_core(k, h).wait_recv()
        other = r.part[src(k), :, quarter(t_x)].astype(F32)
        other = other + r.from_core[k, 1 - half].astype(F32)
        r.part[src(k), :, quarter(t_x)] = other.astype(BF)
        back_x(k).start()

    def sum_x(k):
        back_x(k).wait_recv()
        mine = r.part[src(k), :, quarter(t)].astype(F32)
        mine = mine + r.from_core[k, half].astype(F32)
        return (mine + r.from_x[k].astype(F32)).astype(BF)

    def send_back(k):
        r.part[src(k), :, quarter(t)] = sum_x(k)
        back_ep(k).start()

    def grad_near(k):
        return remote(
            r.dg_send.at[dst(k)],
            r.dg_near.at[k],
            (r.send_dg.at[k], r.recv_dg.at[k]),
            (dst(k % near), t),
        )

    def grad_far(k):
        return remote(
            r.dg_send.at[dst(k)], r.dg_far.at[k], (r.send_dg.at[k], r.recv_dg.at[k]), (dst(k), t)
        )

    close = [k for k in range(n_ep) if k % near]
    far = list(range(near, n_ep, near))

    def grad_sum():
        for k in close:
            grad_near(k).wait_recv()
        for f in [0] + far:
            total = r.dg_send[dst(f)].astype(F32)
            for k in range(f + 1, f + near):
                total = total + r.dg_near[k].astype(F32)
            if f:
                r.dg_send[dst(f)] = total.astype(BF)
                grad_far(f).start()
            else:
                r.dg_in[...] = total[0]
                r.dg_out[...] = total[1]

    def gate_hop(k):
        return remote(
            r.gg_send.at[dst(k)], r.gg_back.at[me], (r.send_gg.at[k], r.recv_gg.at[k]), (dst(k), t)
        )

    own_rows, rank_r = r.in_own.shape
    span = n_ep // n_tp
    block_cols = width // n_ep

    def dense():
        in_whole = r.dense_all[:, :, 0].reshape(width, rank_r)
        out_whole = r.dense_all[:, :, 1].reshape(width, rank_r)
        pre = jnp.dot(r.tok[...], in_whole, preferred_element_type=F32)
        cob = jnp.dot(r.cot[...], out_whole, preferred_element_type=F32)
        gate = r.gate_row[...].astype(F32)
        gate = jnp.concatenate([gate[j : j + 1] for j in range(width // 128)], axis=1)
        r.gate_f32[...] = gate
        gate_wide = jnp.broadcast_to(gate, (16, width)).astype(BF)
        logit = lax.dot_general(
            r.tok[...], gate_wide, CONTRACT_COLS, preferred_element_type=F32
        )[:, :1]
        mix = jax.nn.sigmoid(logit)
        sig = jax.nn.sigmoid(pre)
        act = (pre * sig).astype(BF)
        dpre = (mix * cob * sig * (1.0 + pre * (1.0 - sig))).astype(BF)
        act_wide = act.astype(F32)
        dlogit = mix * (1.0 - mix) * jnp.sum(act_wide * cob, axis=1, keepdims=True)
        in_rows = r.dense_all[pl.ds(t * span, span), :, 0].reshape(cols, rank_r)
        dx = lax.dot_general(dpre, in_rows, CONTRACT_COLS, preferred_element_type=F32)
        r.dense_dx[...] = dx + dlogit * r.gate_f32[:, quarter(t)]
        lane = lax.broadcasted_iota(jnp.int32, (tok_dev, 128), 1)
        high = dlogit.astype(BF).astype(F32)
        low = dlogit - high
        pair = jnp.where(lane == 0, high, jnp.where(lane == 1, low, 0.0)).astype(BF)
        gate_sum = lax.dot_general(pair, r.tok[...], CONTRACT_ROWS, preferred_element_type=F32)
        gate_sum = gate_sum[0:1] + gate_sum[1:2]
        for e in range(n_ep):
            r.gg_send[e, :, :block_cols] = gate_sum[:, e * block_cols : (e + 1) * block_cols]
        mixed = (mix * act_wide).astype(BF)
        for a, (left, right) in enumerate(((r.tok, dpre), (r.cot, mixed))):
            r.grad_gate[:, :rank_r] = lax.dot_general(
                left[...], right, CONTRACT_ROWS, preferred_element_type=F32
            )
            for e in range(n_ep):
                start = pl.multiple_of((e * n_tp + t) * own_rows, own_rows)
                r.dg_send[e, a] = r.grad_gate[
                    pl.ds(start, own_rows), :rank_r
                ].astype(BF)
        r.gg_back[me] = r.gg_send[me]

        @pl.loop(1, n_ep)
        def _(k):
            gate_hop(k).start()

        for k in close:
            grad_near(k).start()

    @pl.loop(0, n_ep + 2)
    def _(n):
        @pl.when(n == 1)
        def _():
            sum_core(0)

        @pl.when(n == 3)
        def _():
            for f in far:
                shard_hop(0, f).wait_recv()
                shard_hop(1, f).start()
                shard_hop(2, f).start()
                for k in range(f + 1, f + near):
                    shard_hop(4, k).start()

        @pl.when((n >= 1) & (n < n_ep))
        def _():
            k = seq(n)
            c = k % near

            @pl.when(c > 0)
            def _():
                for a in range(2):
                    row_hop(a, 0, k).wait_recv()

                    @pl.when(k >= near)
                    def _():
                        row_hop(a, 1, k).start()

                    row_hop(a, 2, k).start()
                w_hop(k).wait_recv()

            @pl.when(c == 0)
            def _():
                i = src(k)
                s = i // near
                for kind in range(2):
                    info_hop(kind, k // near).wait_recv()
                place(s, r.pos, r.weight)
                pick, sent = pick_rows(r.pos, r.weight, me)
                r.w_all[i, :, :cap] = sent
                for a in range(2):

                    @pl.when((inner == 1) & (n == 1))
                    def _():
                        pass_on(a, 1)
                        pass_on(a, 3)

                    @pl.when(inner == 0)
                    def _():
                        raw_hop(a, s, False).wait_recv()

                    rows_all[a][i, :, quarter(t)] = picked(pick, raw[a][s])
                    pick_close(a, k, r.pos, lambda: raw[a][s])
                    row_hop(a, 1, k).start()
                    row_hop(a, 2, k).start()
                    send_close(a, k)

                weigh_close(k, r.pos, r.weight)

        @pl.when(n >= 4)
        def _():
            sum_core(seq(n - 3))

        @pl.when(n == 3)
        def _():
            r.rows_back[me] = sum_x(0)

        @pl.when(n >= 6)
        def _():
            send_back(seq(n - 5))

        @pl.when((n == 0) | (n >= 3))
        def _():
            k = seq(jnp.where(n == 0, 0, n - 2))

            @pl.when(n >= 3)
            def _():
                for a in range(2):
                    for kind in (2, 3):
                        row_hop(a, kind, k).wait_recv()

            run(k)

        @pl.when(n == 0)
        def _():
            @pl.loop(0, n_ep)
            def _(e):
                pick, _ = pick_rows(r.own_pos, r.own_weight, e)
                r.picks[e] = pick

        @pl.when(n == 3)
        def _():
            for f in [0] + far:
                shard_hop(1, f).wait_recv()
                shard_hop(3, f).start()
                for k in range(f + 1, f + near):
                    shard_hop(5, k).start()

        @pl.when(n == 4)
        def _():
            for k in close:
                shard_hop(4, k).wait_recv()
                shard_hop(2, k).start()
                shard_hop(5, k).wait_recv()
                shard_hop(3, k).start()

        @pl.when((n >= 2) & (n < n_ep + 1))
        def _():
            k = seq(n - 1)
            for a in range(2):
                row_hop(a, 1, k).wait_recv()
                row_hop(a, 3, k).start()

        @pl.when(n == 6)
        def _():
            grad_sum()

        @pl.when((inner == 1) & (n == near + 1))
        def _():
            for a in range(2):
                pass_on(a, 2)

        @pl.when(n == 5)
        def _():
            @pl.loop(0, n_ep)
            def _(k):
                for kind in (2, 3):
                    shard_hop(kind, k).wait_recv()

            dense()

    rows = n_ep * cap
    tiles = width // cols

    def tile(kind, j):
        if kind == 0:
            r.grad_down[:, quarter(j)] = lax.dot_general(
                r.act[...].reshape(rows, -1),
                r.dy_all.reshape(rows, width)[:, quarter(j)],
                CONTRACT_ROWS,
                preferred_element_type=F32,
            )
            return
        out, right = ((r.grad_gate, r.d_gate), (r.grad_up, r.d_up))[kind - 1]
        out[quarter(j), :] = lax.dot_general(
            r.x_all.reshape(rows, width)[:, quarter(j)],
            right[...].reshape(rows, -1),
            CONTRACT_ROWS,
            preferred_element_type=F32,
        )

    def weight_core():
        return remote(r.w_part, r.w_from.at[0], (r.send_wt.at[0], r.recv_wt.at[0]), core_peer)

    def weight_x():
        return remote(r.w_half, r.w_from.at[1], (r.send_wt.at[1], r.recv_wt.at[1]), x_peer)

    def weight_ep(k):
        return remote(
            r.w_sum.at[src(k)], r.w_back.at[me], (r.send_we.at[k], r.recv_we.at[k]), (src(k), t)
        )

    weight_core().start()
    send_back(seq(n_ep - 3))
    tile(0, 0)
    sum_core(seq(n_ep - 1))
    weight_core().wait_recv()
    r.w_half[...] = r.w_part[...] + r.w_from[0]
    send_back(seq(n_ep - 2))
    weight_x().start()
    for j in range(1, tiles):
        tile(0, j)
    weight_x().wait_recv()
    r.w_sum[...] = r.w_half[...] + r.w_from[1]
    send_back(seq(n_ep - 1))
    r.w_back[me] = r.w_sum[me]

    @pl.loop(1, n_ep)
    def _(k):
        weight_ep(k).start()

    for kind in (1, 2):
        for j in range(tiles):
            tile(kind, j)

    @pl.loop(1, n_ep)
    def _(k):
        gate_hop(k).wait_recv()

    for f in far:
        grad_far(f).wait_recv()
        r.dg_in[...] += r.dg_far[f, 0].astype(F32)
        r.dg_out[...] += r.dg_far[f, 1].astype(F32)
    gate_total = jnp.zeros(r.gg_back.shape[1:], F32)
    for e in range(n_ep):
        gate_total = gate_total + r.gg_back[e]
    block = block_cols // n_tp
    r.gg_out[...] = sum(
        jnp.where(t == q, gate_total[:, q * block : (q + 1) * block], 0.0) for q in range(n_tp)
    )

    @pl.loop(1, n_ep)
    def _(k):
        weight_ep(k).wait_recv()
        back_ep(k).wait_recv()

    picks = r.picks[...].reshape(rows, tok_dev)
    moved = lax.dot_general(
        picks,
        r.rows_back[...].reshape(rows, cols),
        CONTRACT_ROWS,
        preferred_element_type=F32,
    )
    r.grad_tokens[...] = (r.dense_dx[...] + moved).astype(BF)
    found = [jnp.zeros((1, tok_dev), F32) for _ in range(top_k)]
    for e in range(n_ep):
        row = r.w_back[e]
        row = jnp.broadcast_to(row, (16, lanes)).astype(BF)[:, :cap]
        spread = jnp.dot(row, r.picks[e], preferred_element_type=F32)[0:1]
        for k in range(top_k):
            found[k] = found[k] + jnp.where(r.ids[k : k + 1, :] == e, spread, 0.0)
    for k in range(top_k):
        r.grad_route[k : k + 1, :] = found[k].astype(BF)

    for f in [0] + far:
        shard_hop(1, f).wait_send()
    for f in far:
        shard_hop(0, f).wait_send()
        grad_far(f).wait_send()
    for f in range(1, planes):
        for kind in range(2):
            info_hop(kind, f).wait_send()
    for a in range(2):
        each_own(a, lambda c: c.wait_send())
        for s in range(planes):
            each_raw(a, s, lambda c: c.wait_send())
    for k in close:
        w_hop(k).wait_send()
        for a in range(2):
            row_hop(a, 0, k).wait_send()
        shard_hop(4, k).wait_send()
        shard_hop(5, k).wait_send()
        grad_near(k).wait_send()

    @pl.loop(0, n_ep)
    def _(k):
        for kind in (2, 3):
            shard_hop(kind, k).wait_send()
        for h in range(2):
            back_core(k, h).wait_send()
        back_x(k).wait_send()

    @pl.loop(1, n_ep)
    def _(k):
        for a in range(2):
            for kind in range(1, 4):
                row_hop(a, kind, k).wait_send()
        back_ep(k).wait_send()
        weight_ep(k).wait_send()
        gate_hop(k).wait_send()

    weight_core().wait_send()
    weight_x().wait_send()


def store_kernel(count, *refs):
    copies = [
        pltpu.make_async_copy(refs[n], refs[count + n], refs[2 * count].at[n])
        for n in range(count)
    ]
    for c in copies:
        c.start()
    for c in copies:
        c.wait()


def store(arrays):
    return pl.pallas_call(
        functools.partial(store_kernel, len(arrays)),
        out_shape=tuple(jax.ShapeDtypeStruct(a.shape, a.dtype) for a in arrays),
        in_specs=[VMEM] * len(arrays),
        out_specs=(ANY,) * len(arrays),
        scratch_shapes=[pltpu.SemaphoreType.DMA((len(arrays),))],
        compiler_params=pltpu.CompilerParams(vmem_limit_bytes=16 * 1024 * 1024),
        name="store",
    )(*arrays)


def shards(
    tokens,
    cotangent,
    route_ids,
    route_weights,
    w_gate,
    w_up,
    w_down,
    dense_in,
    dense_out,
    dense_gate,
):
    n_ep = lax.axis_size("ep")
    n_tp = lax.axis_size("tp")
    tok_dev, width = tokens.shape
    top_k = route_ids.shape[1]
    cols = width // n_tp
    near = n_ep // 4
    cap = 2 * tok_dev * top_k // n_ep
    lanes = -(-cap // 128) * 128
    hidden = w_gate.shape[2]
    own_rows, rank_r = dense_in.shape
    gate_lanes = -(-(width // n_ep) // 128) * 128
    dma = pltpu.SemaphoreType.DMA
    args = dict(
        ids=(route_ids.T, VMEM),
        route=(route_weights.T, VMEM),
        gate_row=(dense_gate.reshape(-1, 128), VMEM),
        tokens=(tokens, ANY),
        cotangent=(cotangent, ANY),
        in_own=(dense_in, ANY),
        out_own=(dense_out, ANY),
        w_gate=(w_gate[0], ANY),
        w_up=(w_up[0], ANY),
        w_down=(w_down[0], ANY),
    )
    outs = dict(
        grad_tokens=((tok_dev, cols), BF),
        grad_route=((top_k, tok_dev), BF),
        grad_gate=((width, hidden), F32),
        grad_up=((width, hidden), F32),
        grad_down=((hidden, width), F32),
        dg_in=((own_rows, rank_r), F32),
        dg_out=((own_rows, rank_r), F32),
        gg_out=((1, width // (n_ep * n_tp)), F32),
    )
    scratch = dict(
        tok=((tok_dev, width), BF),
        cot=((tok_dev, width), BF),
        gate_w=((width, hidden), BF),
        up_w=((width, hidden), BF),
        down_w=((hidden, width), BF),
        own_pos=((max(16, n_ep), tok_dev), F32),
        own_weight=((max(16, n_ep), tok_dev), F32),
        pos=((max(16, n_ep), tok_dev), F32),
        weight=((max(16, n_ep), tok_dev), F32),
        below=((tok_dev, tok_dev), BF),
        ids_all=((4, top_k, tok_dev), jnp.int32),
        route_all=((4, top_k, tok_dev), F32),
        x_extra=((near, cap, cols), BF),
        dy_extra=((near, cap, cols), BF),
        x_raw=((4, tok_dev, cols), BF),
        dy_raw=((4, tok_dev, cols), BF),
        picks=((n_ep, cap, tok_dev), BF),
        w_send=((n_ep, 1, lanes), F32),
        w_all=((n_ep, 1, lanes), F32),
        x_send=((n_ep, cap, cols), BF),
        dy_send=((n_ep, cap, cols), BF),
        x_all=((n_ep, cap, width), BF),
        dy_all=((n_ep, cap, width), BF),
        act=((n_ep, cap, hidden), BF),
        d_gate=((n_ep, cap, hidden), BF),
        d_up=((n_ep, cap, hidden), BF),
        part=((n_ep, cap, width), BF),
        w_part=((n_ep, 1, lanes), F32),
        from_core=((n_ep, 2, cap, cols), BF),
        from_x=((n_ep, cap, cols), BF),
        rows_back=((n_ep, cap, cols), BF),
        dense_all=((n_ep, n_tp, 2, own_rows, rank_r), BF),
        dense_dx=((tok_dev, cols), F32),
        gate_f32=((1, width), F32),
        dg_send=((n_ep, 2, own_rows, rank_r), BF),
        dg_near=((n_ep, 2, own_rows, rank_r), BF),
        dg_far=((n_ep, 2, own_rows, rank_r), BF),
        gg_send=((n_ep, 1, gate_lanes), F32),
        gg_back=((n_ep, 1, gate_lanes), F32),
        w_from=((2, n_ep, 1, lanes), F32),
        w_half=((n_ep, 1, lanes), F32),
        w_sum=((n_ep, 1, lanes), F32),
        w_back=((n_ep, 1, lanes), F32),
    )
    sems = dict(
        load_sem=(7,),
        send_info=(2, 4),
        recv_info=(2, 4),
        send_raw=(2, 2, 4),
        recv_raw=(2, 4),
        send_rows=(2, 4, n_ep),
        recv_rows=(2, 4, n_ep),
        send_shard=(6, n_ep),
        recv_shard=(6, n_ep),
        send_w=(n_ep,),
        recv_w=(n_ep,),
        send_bc=(n_ep, 2),
        recv_bc=(n_ep, 2),
        send_bx=(n_ep,),
        recv_bx=(n_ep,),
        send_be=(n_ep,),
        recv_be=(n_ep,),
        send_dg=(n_ep,),
        recv_dg=(n_ep,),
        send_gg=(n_ep,),
        recv_gg=(n_ep,),
        send_wt=(2,),
        recv_wt=(2,),
        send_we=(n_ep,),
        recv_we=(n_ep,),
    )
    names = list(args) + list(outs) + list(scratch) + list(sems)
    results = pl.pallas_call(
        functools.partial(layer_kernel, n_ep, n_tp, names),
        out_shape=tuple(pltpu.VMEM(s, d) for s, d in outs.values()),
        in_specs=[spec for _, spec in args.values()],
        out_specs=(VMEM,) * len(outs),
        scratch_shapes=[pltpu.VMEM(s, d) for s, d in scratch.values()]
        + [dma(s) for s in sems.values()],
        compiler_params=pltpu.CompilerParams(
            collective_id=0, has_side_effects=True, vmem_limit_bytes=48 * 1024 * 1024
        ),
        name="layer",
    )(*(a for a, _ in args.values()))
    grad_tokens, grad_route, grad_gate, grad_up, grad_down, dg_in, dg_out, gg_out = store(results)
    return (
        grad_tokens,
        grad_route.T,
        grad_gate[None],
        grad_up[None],
        grad_down[None],
        dg_in,
        dg_out,
        gg_out[0],
    )


def solution(mesh):
    placed = (
        P("ep", None),
        P("ep", None),
        P("ep", None),
        P("ep", None),
        P("ep", None, "tp"),
        P("ep", None, "tp"),
        P("ep", "tp", None),
        P(("ep", "tp"), None),
        P(("ep", "tp"), None),
        P(),
    )
    return jax.shard_map(
        shards,
        mesh=mesh,
        in_specs=placed,
        out_specs=(
            P("ep", "tp"),
            P("ep", None),
            P("ep", None, "tp"),
            P("ep", None, "tp"),
            P("ep", "tp", None),
            P(("ep", "tp"), None),
            P(("ep", "tp"), None),
            P(("ep", "tp")),
        ),
        check_vma=False,
    )
```
